128 devices in a mesh: ep: 128 (over z, y, x, core).
Axes of the slice: x: 4, y: 4, z: 4, core: 2. Of those that a mesh axis runs over, the one named last changes fastest.
Arguments:
- residual: bfloat16 [8192, 2048], P('ep'), may hold values from -6 to 6
- branch_in: bfloat16 [8192, 1024], P('ep'), may hold values from -6 to 6
- state_real: float32 [8192, 4096], P('ep'), may hold values from -4 to 4
- state_imag: float32 [8192, 4096], P('ep'), may hold values from -4 to 4
- decay_rate: float32 [64, 64], replicated, may hold values from 0.1 to 1
- frequency: float32 [64, 64], replicated, may hold values from 0 to 200
- log_step: float32 [64], replicated, may hold values from -4 to 0
- input_real: bfloat16 [64, 64, 16], replicated, may hold values from -1 to 1
- input_imag: bfloat16 [64, 64, 16], replicated, may hold values from -1 to 1
- output_matrix_real: bfloat16 [64, 16, 64], replicated, may hold values from -0.5 to 0.5
- output_matrix_imaginary: bfloat16 [64, 16, 64], replicated, may hold values from -0.5 to 0.5
- skip_gain: float32 [1024], replicated, may hold values from -4 to 4
- glu_value: bfloat16 [1024, 2048], replicated, may hold values from -0.1875 to 0.1875
- glu_gate: bfloat16 [1024, 2048], replicated, may hold values from -0.1875 to 0.1875
- mix_gain: float32 [2048], replicated, may hold values from 0.1 to 1.9
- moe_in_gain: float32 [2048], replicated, may hold values from 0.1 to 1.9
- moe_out_gain: float32 [2048], replicated, may hold values from 0.1 to 1.9
- routes: int32 [8192, 6], P('ep'), may hold values from 0 to 127, all different within a row; in each aligned block of 64 rows (0 to 63, 64 to 127, ...) at most 4 rows name the same one
- route_weights: float32 [8192, 6], P('ep'), may hold values from 0.05 to 0.6
- expert_gate: bfloat16 [128, 2048, 512], P('ep'), may hold values from -0.125 to 0.125
- expert_up: bfloat16 [128, 2048, 512], P('ep'), may hold values from -0.125 to 0.125
- expert_down: bfloat16 [128, 512, 2048], P('ep'), may hold values from -0.25 to 0.25
- shared_gate: bfloat16 [2048, 512], replicated, may hold values from -0.125 to 0.125
- shared_up: bfloat16 [2048, 512], replicated, may hold values from -0.125 to 0.125
- shared_down: bfloat16 [512, 2048], replicated, may hold values from -0.25 to 0.25
Outputs:
- layer_out: bfloat16 [8192, 2048], P('ep')
- next_real: float32 [8192, 4096], P('ep')
- next_imag: float32 [8192, 4096], P('ep')
The draws below stay inside these ranges and needn't reach their ends.
Inputs may be any that keep to these rules, and one draw needn't show every extreme that they name: `routes`: among the rows of one device no expert is named more than 4 times, and in every draw some expert is named exactly 4 times by some device's rows; a token's experts are distinct.
All inputs are finite; a program needn't handle non-finite values.
Results may differ from the reference program's by a relative error of at most 0.0066.
Values may be sent and summed in bfloat16 or wider, within the bound.
A program may use at most 128 MiB of HBM per device.

```python
import math
import jax
import jax.numpy as jnp
import numpy as np
from jax import lax

D = 2048
SSM_W = 1024
GCH = 16
GROUPS = 64
STATE = 64
EH = 512
TOP_K = 6
SEQ_DEV = 64
SEQS = 8192
EXPERTS = 128
CAP = 4
N_EP = 128


def levels(key, shape, pieces, least, largest):
    def one(dim, shards_of):
        steps = jax.random.uniform(jax.random.fold_in(jax.random.fold_in(key, 6), dim), (shards_of,), jnp.float32, least / len(pieces), largest / len(pieces))
        return jnp.repeat(jnp.exp(steps), shape[dim] // shards_of).reshape((-1,) + (1,) * (len(shape) - dim - 1))

    factor_of = one(*pieces[0])
    for cut in pieces[1:]:
        factor_of = factor_of * one(*cut)
    return factor_of


def shared_out(key, own, number, rows, amount, top, most, lean):
    ranking = jax.random.permutation(key, amount)
    heavy_load, ordinary = portions_of(amount, rows * top, most, lean, True), portions_of(amount, rows * top, most, lean, False)
    places = jnp.arange(amount)

    def named(sizes, rotation):
        used = int((sizes > 0).sum())
        fixed = max(1, used // 4)
        moved = fixed + (places - fixed + rotation * (used - fixed)) % max(1, amount - fixed)
        return jnp.zeros((amount,), jnp.int32).at[ranking[jnp.where(places < fixed, places, moved)]].set(jnp.asarray(sizes, jnp.int32))

    sizes = jnp.where(number % 4 == 0, named(heavy_load, number // 4), named(ordinary, number - number // 4 - 1))
    mixed = jax.random.permutation(jax.random.fold_in(own, 3), amount)
    source_of, sink = mixed[0:amount // 2 * 2:2], mixed[1:amount // 2 * 2:2]
    slack = jnp.minimum(sizes[source_of] - 1, most - sizes[sink]) // 2
    slack = jnp.where((source_of == ranking[0]) | (sink == ranking[0]) | (sizes[sink] == 0), 0, jnp.maximum(slack, 0))
    moved = jax.random.randint(jax.random.fold_in(own, 4), (amount // 2,), 0, 1 << 20) % (slack + 1)
    sizes = sizes.at[source_of].add(-moved).at[sink].add(moved)
    items = jnp.searchsorted(jnp.cumsum(sizes), jnp.arange(rows * top), side="right").astype(jnp.int32)
    table = items.reshape(top, rows).T
    table = table[jax.random.permutation(jax.random.fold_in(own, 1), rows)]
    rotation = jax.random.randint(jax.random.fold_in(own, 2), (rows, 1), 0, top)
    return jnp.take_along_axis(table, (jnp.arange(top)[None, :] + rotation) % top, axis=1)


def portions_of(amount, total, reach, skew, full):
    weights = [(1 << 20) // math.isqrt(rank ** skew) + 1 for rank in range(1, amount + 1)]
    largest = reach if full else min(reach, max(-(-total // amount), total * weights[0] // sum(weights)))
    least = 1 if total - largest >= amount - 1 else 0
    given, surplus = [largest] + [least] * (amount - 1), total - largest - least * (amount - 1)
    while surplus > 0:
        candidates = [i for i in range(1, amount) if given[i] < largest] or [i for i in range(1, amount) if given[i] < reach]
        whole, left = sum([weights[i] for i in candidates]), surplus
        for i in candidates:
            more = min(reach - given[i], max(1, left * weights[i] // whole), surplus)
            given[i] = given[i] + more
            surplus = surplus - more
    return np.array(given)


def bell_draw(rng, shape, deviation, reach, split=(), kind=jnp.bfloat16):
    loudness = levels(rng, shape, split, -0.22, 0.18) if split else 1.0
    array = jax.random.normal(rng, shape, jnp.float32) * deviation * loudness
    return jnp.minimum(jnp.maximum(array, -reach), reach).astype(kind)


def setup_inputs(seed: int = 0) -> dict:
    arg_keys = jax.random.split(jax.random.key(seed), 26)
    residual = bell_draw(arg_keys[0], (SEQS, D), 1.0, 6.0, ((0, 128),))
    branch_in = bell_draw(arg_keys[1], (SEQS, SSM_W), 1.0, 6.0, ((0, 128),))
    state_real = bell_draw(arg_keys[2], (SEQS, GROUPS * STATE), 0.5, 4.0, ((0, 128),), jnp.float32)
    state_imag = bell_draw(arg_keys[3], (SEQS, GROUPS * STATE), 0.5, 4.0, ((0, 128),), jnp.float32)
    decay_rate = jnp.clip(jnp.exp(jax.random.uniform(arg_keys[4], (GROUPS, STATE), jnp.float32, math.log(0.1), math.log(1.0))), 0.1, 1.0)
    frequency = jnp.clip(jax.random.uniform(arg_keys[5], (GROUPS, STATE), jnp.float32, 0.0, 200.0), 0.0, 200.0)
    log_step = jnp.clip(jax.random.uniform(arg_keys[6], (GROUPS,), jnp.float32, -4.0, 0.0), -4.0, 0.0)
    input_real = bell_draw(arg_keys[7], (GROUPS, STATE, GCH), (2 * GCH) ** -0.5, 1.0)
    input_imag = bell_draw(arg_keys[8], (GROUPS, STATE, GCH), (2 * GCH) ** -0.5, 1.0)
    output_matrix_real = bell_draw(arg_keys[9], (GROUPS, GCH, STATE), (2 * STATE) ** -0.5, 0.5)
    output_matrix_imaginary = bell_draw(arg_keys[10], (GROUPS, GCH, STATE), (2 * STATE) ** -0.5, 0.5)
    skip_gain = bell_draw(arg_keys[11], (SSM_W,), 1.0, 4.0, (), jnp.float32)
    glu_value = bell_draw(arg_keys[12], (SSM_W, D), SSM_W ** -0.5, 0.1875)
    glu_gate = bell_draw(arg_keys[13], (SSM_W, D), SSM_W ** -0.5, 0.1875)
    mix_gain = jnp.clip(1.0 + 0.18 * jax.random.normal(arg_keys[14], (D,), jnp.float32), 0.1, 1.9)
    moe_in_gain = jnp.clip(1.0 + 0.18 * jax.random.normal(arg_keys[15], (D,), jnp.float32), 0.1, 1.9)
    moe_out_gain = jnp.clip(1.0 + 0.18 * jax.random.normal(arg_keys[16], (D,), jnp.float32), 0.1, 1.9)
    routes_keys = jax.random.split(jax.random.fold_in(arg_keys[17], 1), SEQS // SEQ_DEV)
    routes_turns = jax.random.permutation(jax.random.fold_in(arg_keys[17], 3), SEQS // SEQ_DEV)
    routes = jax.vmap(lambda own, number: shared_out(jax.random.fold_in(arg_keys[17], 2), own, number, SEQ_DEV, EXPERTS, TOP_K, CAP, 2))(routes_keys, routes_turns).reshape((SEQS, TOP_K))
    route_weights = jnp.clip(0.05 + 0.55 * jax.random.uniform(arg_keys[18], (SEQS, TOP_K), jnp.float32) ** levels(arg_keys[18], (SEQS, TOP_K), ((0, 128),), -0.2, 0.2), 0.05, 0.6)
    expert_gate = bell_draw(arg_keys[19], (EXPERTS, D, EH), D ** -0.5, 0.125, ((0, 128),))
    expert_up = bell_draw(arg_keys[20], (EXPERTS, D, EH), D ** -0.5, 0.125, ((0, 128),))
    expert_down = bell_draw(arg_keys[21], (EXPERTS, EH, D), EH ** -0.5, 0.25, ((0, 128),))
    shared_gate = bell_draw(arg_keys[22], (D, EH), D ** -0.5, 0.125)
    shared_up = bell_draw(arg_keys[23], (D, EH), D ** -0.5, 0.125)
    shared_down = bell_draw(arg_keys[24], (EH, D), EH ** -0.5, 0.25)
    return dict(residual=residual, branch_in=branch_in, state_real=state_real, state_imag=state_imag, decay_rate=decay_rate, frequency=frequency, log_step=log_step, input_real=input_real, input_imag=input_imag, output_matrix_real=output_matrix_real, output_matrix_imaginary=output_matrix_imaginary, skip_gain=skip_gain, glu_value=glu_value, glu_gate=glu_gate, mix_gain=mix_gain, moe_in_gain=moe_in_gain, moe_out_gain=moe_out_gain, routes=routes, route_weights=route_weights, expert_gate=expert_gate, expert_up=expert_up, expert_down=expert_down, shared_gate=shared_gate, shared_up=shared_up, shared_down=shared_down)


norm_eps = 1e-06

def scaled_norm(row_block, norm_gain):
    return row_block * lax.rsqrt(lax.optimization_barrier(jnp.mean(row_block * row_block, axis=-1, keepdims=True)) + norm_eps) * norm_gain

def state_step(branch_in, state_real, state_imag, decay_rate, frequency, log_step, input_real, input_imag, output_matrix_real, output_matrix_imaginary, skip_gain):
    seq_count = branch_in.shape[0]
    group_count, state_count = decay_rate.shape
    chan_count = input_real.shape[2]
    step_size = jnp.exp(log_step)[:, None]
    magnitude = jnp.exp(-decay_rate * step_size)
    abar_re = magnitude * jnp.cos(frequency * step_size)
    abar_im = magnitude * jnp.sin(frequency * step_size)
    lam_re = -decay_rate
    lam_im = frequency
    denominator = lam_re * lam_re + lam_im * lam_im
    numer_re = abar_re - 1.0
    coef_re = (numer_re * lam_re + abar_im * lam_im) / denominator
    coef_im = (abar_im * lam_re - numer_re * lam_im) / denominator
    b_real = input_real.astype(jnp.float32)
    b_imag = input_imag.astype(jnp.float32)
    bbar_re = coef_re[..., None] * b_real - coef_im[..., None] * b_imag
    bbar_im = coef_re[..., None] * b_imag + coef_im[..., None] * b_real
    feed_rows = branch_in.astype(jnp.float32).reshape(seq_count, group_count, chan_count)
    forcing_real = jnp.einsum('tgc,gpc->tgp', feed_rows, bbar_re, precision=lax.Precision.HIGHEST)
    drive_im = jnp.einsum('tgc,gpc->tgp', feed_rows, bbar_im, precision=lax.Precision.HIGHEST)
    old_re = state_real.reshape(seq_count, group_count, state_count)
    old_im = state_imag.reshape(seq_count, group_count, state_count)
    fresh_real = abar_re * old_re - abar_im * old_im + forcing_real
    fresh_imaginary = abar_re * old_im + abar_im * old_re + drive_im
    state_readout = jnp.einsum('ukb,krb->ukr', fresh_real, output_matrix_real.astype(jnp.float32), precision=lax.Precision.HIGHEST) - jnp.einsum('ukb,krb->ukr', fresh_imaginary, output_matrix_imaginary.astype(jnp.float32), precision=lax.Precision.HIGHEST)
    mixed_rows = state_readout.reshape(seq_count, group_count * chan_count) + skip_gain * branch_in.astype(jnp.float32)
    activated = jax.nn.gelu(mixed_rows).astype(jnp.bfloat16)
    return (activated, fresh_real.reshape(seq_count, -1), fresh_imaginary.reshape(seq_count, -1))

def expert_rows(row_block, w_gate, w_up, w_down):
    gate_part = jnp.dot(row_block, w_gate, preferred_element_type=jnp.float32)
    up_part = jnp.dot(row_block, w_up, preferred_element_type=jnp.float32)
    hidden = (jax.nn.silu(gate_part) * up_part).astype(jnp.bfloat16)
    return jnp.dot(hidden, w_down, preferred_element_type=jnp.float32)

def mixer_residual(residual, activated, glu_value, glu_gate, mix_gain):
    value_part = jnp.dot(activated, glu_value, preferred_element_type=jnp.float32)
    gate_part = jnp.dot(activated, glu_gate, preferred_element_type=jnp.float32)
    branch = value_part * jax.nn.sigmoid(gate_part)
    return (residual.astype(jnp.float32) + scaled_norm(branch, mix_gain)).astype(jnp.bfloat16)

def reference(residual, branch_in, state_real, state_imag, decay_rate, frequency, log_step, input_real, input_imag, output_matrix_real, output_matrix_imaginary, skip_gain, glu_value, glu_gate, mix_gain, moe_in_gain, moe_out_gain, routes, route_weights, expert_gate, expert_up, expert_down, shared_gate, shared_up, shared_down):
    activated, next_real, next_imag = state_step(branch_in, state_real, state_imag, decay_rate, frequency, log_step, input_real, input_imag, output_matrix_real, output_matrix_imaginary, skip_gain)
    resid_mid = mixer_residual(residual, activated, glu_value, glu_gate, mix_gain)
    normed = scaled_norm(resid_mid.astype(jnp.float32), moe_in_gain).astype(jnp.bfloat16)
    hidden_width = normed.shape[1]
    flat_routes = routes.reshape(-1).astype(jnp.int32)
    assign_count = flat_routes.shape[0]
    sorted_order = jnp.argsort(flat_routes, stable=True).astype(jnp.int32)
    sorted_expert = flat_routes[sorted_order]
    expert_load = lax.optimization_barrier(jnp.sum((flat_routes[:, None] == jnp.arange(EXPERTS, dtype=jnp.int32)[None, :]).astype(jnp.int32), axis=0))
    load_start = jnp.cumsum(expert_load) - expert_load
    slot_rank = jnp.arange(assign_count, dtype=jnp.int32) - load_start[sorted_expert]
    slot_most = CAP * N_EP
    slot_index = (sorted_expert * slot_most + slot_rank).astype(jnp.int32)
    slot_table = jnp.full((EXPERTS * slot_most,), SEQS, jnp.int32).at[slot_index].set(sorted_order // TOP_K)
    padded = jnp.concatenate([normed, jnp.zeros((1, hidden_width), jnp.bfloat16)], axis=0)

    def one_expert(expert_args):
        row_ids, w_gate, w_up, w_down = expert_args
        return expert_rows(padded[row_ids], w_gate, w_up, w_down).astype(jnp.bfloat16)
    expert_out = lax.map(one_expert, (slot_table.reshape(EXPERTS, slot_most), expert_gate, expert_up, expert_down))
    assign_slot = jnp.zeros((assign_count,), jnp.int32).at[sorted_order].set(slot_index)
    per_assign = expert_out.reshape(-1, hidden_width)[assign_slot].reshape(SEQS, TOP_K, hidden_width).astype(jnp.float32)
    routed = lax.optimization_barrier(jnp.sum(per_assign * route_weights[..., None], axis=1))
    shared = expert_rows(normed, shared_gate, shared_up, shared_down)
    combined = shared + routed
    layer_out = (resid_mid.astype(jnp.float32) + scaled_norm(combined, moe_out_gain)).astype(jnp.bfloat16)
    return (layer_out, next_real, next_imag)
```

```python
import functools

import jax
import jax.numpy as jnp
from jax import lax
from jax.experimental import pallas as pl
from jax.experimental.pallas import tpu as pltpu
from jax.sharding import PartitionSpec as P

MESH = pl.DeviceIdType.MESH
F32 = jnp.float32
BF16 = jnp.bfloat16
EPS = 1e-06
N_DEV = 128
CAP = 4
SLOTS = N_DEV * CAP
STRIDE = 43
STRIDE_INV = pow(STRIDE, -1, N_DEV)
GROUPS = 4
GROUP_DEV = N_DEV // GROUPS
GROUP_ROWS = SLOTS // GROUPS
NT = (((1,), (1,)), ((), ()))
TN = (((0,), (0,)), ((), ()))


def split_hi_lo(value):
    hi = value.astype(BF16)
    lo = (value - hi.astype(F32)).astype(BF16)
    return hi, lo


SSM_STEPS = 4
BLOCKS_PER_STEP = 8 // SSM_STEPS


def state_kernel(
    feed_ref,
    re_ref,
    im_ref,
    decay_ref,
    freq_ref,
    log_step_ref,
    in_re_ref,
    in_im_ref,
    out_re_ref,
    out_im_ref,
    skip_ref,
    next_re_ref,
    next_im_ref,
    act_ref,
):
    step = pl.program_id(0)
    rows = 8 * BLOCKS_PER_STEP
    group = lax.broadcasted_iota(jnp.int32, (rows, 64), 0) + step * rows
    lane = lax.broadcasted_iota(jnp.int32, (rows, 64), 1)
    column = jnp.sum(
        jnp.where(group == lane, jnp.broadcast_to(log_step_ref[...], (rows, 64)), 0.0),
        axis=1,
        keepdims=True,
    )
    step_size = jnp.exp(column)
    decay = decay_ref[...]
    freq = freq_ref[...]
    magnitude = jnp.exp(-decay * step_size)
    phase = freq * step_size
    abar_re = magnitude * jnp.cos(phase)
    abar_im = magnitude * jnp.sin(phase)
    denominator = decay * decay + freq * freq
    numer_re = abar_re - 1.0
    coef_re = (abar_im * freq - numer_re * decay) / denominator
    coef_im = (-abar_im * decay - numer_re * freq) / denominator

    def twice(v):
        return jnp.concatenate([v, v], axis=1)

    abar_re, abar_im, coef_re, coef_im = map(
        twice, (abar_re, abar_im, coef_re, coef_im)
    )
    row_group = lax.broadcasted_iota(jnp.int32, (128, 128), 0) // 16
    lane_half = lax.broadcasted_iota(jnp.int32, (128, 128), 1) // 64
    low_half = lax.broadcasted_iota(jnp.int32, (1, 128), 1) < 64
    for b in range(BLOCKS_PER_STEP):
        bb_re, bb_im = [], []
        for g in range(8):
            r = b * 8 + g
            own = slice(r * 16, r * 16 + 16)
            b_re = twice(in_re_ref[own, :].astype(F32))
            b_im = twice(in_im_ref[own, :].astype(F32))
            c_re, c_im = coef_re[r : r + 1, :], coef_im[r : r + 1, :]
            bb_re.append(c_re * b_re - c_im * b_im)
            bb_im.append(c_re * b_im + c_im * b_re)
        bb_re = jnp.concatenate(bb_re, axis=0)
        bb_im = jnp.concatenate(bb_im, axis=0)
        rows_here = slice(b * 128, b * 128 + 128)
        o_re = twice(out_re_ref[rows_here, :].astype(F32))
        o_im = twice(-out_im_ref[rows_here, :].astype(F32))
        parts_re_hi, parts_re_lo = split_hi_lo(bb_re)
        parts_im_hi, parts_im_lo = split_hi_lo(bb_im)
        feed = feed_ref[:, b * 128 : b * 128 + 128]
        feed_twice = jnp.concatenate([feed, feed], axis=1)
        readout = jnp.zeros((64, 128), F32)
        for q in range(4):
            mask = row_group == 2 * q + lane_half
            zero = jnp.zeros((128, 128), BF16)

            def block(hi, lo):
                return jnp.concatenate(
                    [jnp.where(mask, hi, zero), jnp.where(mask, lo, zero)], axis=0
                )

            f_re = jnp.dot(
                feed_twice, block(parts_re_hi, parts_re_lo), preferred_element_type=F32
            )
            f_im = jnp.dot(
                feed_twice, block(parts_im_hi, parts_im_lo), preferred_element_type=F32
            )
            r0 = b * 8 + 2 * q
            a_re = jnp.where(
                low_half, abar_re[r0 : r0 + 1, :], abar_re[r0 + 1 : r0 + 2, :]
            )
            a_im = jnp.where(
                low_half, abar_im[r0 : r0 + 1, :], abar_im[r0 + 1 : r0 + 2, :]
            )
            lanes = slice(b * 512 + q * 128, b * 512 + q * 128 + 128)
            old_re, old_im = re_ref[:, lanes], im_ref[:, lanes]
            new_re = a_re * old_re - a_im * old_im + f_re
            new_im = a_re * old_im + a_im * old_re + f_im
            next_re_ref[:, lanes] = new_re
            next_im_ref[:, lanes] = new_im
            re_hi, re_lo = split_hi_lo(new_re)
            im_hi, im_lo = split_hi_lo(new_im)
            w = jnp.concatenate(
                [
                    jnp.where(mask, o_re, 0.0).astype(BF16),
                    jnp.where(mask, o_im, 0.0).astype(BF16),
                ],
                axis=1,
            )
            left = jnp.concatenate(
                [
                    jnp.concatenate([re_hi, im_hi], axis=1),
                    jnp.concatenate([re_lo, im_lo], axis=1),
                ],
                axis=0,
            )
            both = lax.dot_general(left, w, NT, preferred_element_type=F32)
            readout = readout + (both[:64] + both[64:])
        here = slice(b * 128, b * 128 + 128)
        mixed = readout + skip_ref[:, here] * feed.astype(F32)
        act_ref[:, here] = jax.nn.gelu(mixed).astype(BF16)


def state_step(
    branch_in,
    state_real,
    state_imag,
    decay_rate,
    frequency,
    log_step,
    input_real,
    input_imag,
    output_matrix_real,
    output_matrix_imaginary,
    skip_gain,
):
    in_re = jnp.transpose(input_real, (0, 2, 1)).reshape(1024, 64)
    in_im = jnp.transpose(input_imag, (0, 2, 1)).reshape(1024, 64)
    out_re = output_matrix_real.reshape(1024, 64)
    out_im = output_matrix_imaginary.reshape(1024, 64)
    n = SSM_STEPS
    wide = pl.BlockSpec((64, 4096 // n), lambda i: (0, i))
    narrow = pl.BlockSpec((64, 1024 // n), lambda i: (0, i))
    per_group = pl.BlockSpec((64 // n, 64), lambda i: (i, 0))
    per_channel = pl.BlockSpec((1024 // n, 64), lambda i: (i, 0))
    return pl.pallas_call(
        state_kernel,
        grid=(n,),
        out_shape=(
            jax.ShapeDtypeStruct((64, 4096), F32),
            jax.ShapeDtypeStruct((64, 4096), F32),
            jax.ShapeDtypeStruct((64, 1024), BF16),
        ),
        in_specs=[
            narrow,
            wide,
            wide,
            per_group,
            per_group,
            pl.BlockSpec((1, 64), lambda i: (0, 0)),
            per_channel,
            per_channel,
            per_channel,
            per_channel,
            pl.BlockSpec((1, 1024 // n), lambda i: (0, i)),
        ],
        out_specs=(wide, wide, narrow),
        compiler_params=pltpu.CompilerParams(
            dimension_semantics=("arbitrary",), vmem_limit_bytes=20 * 2**20
        ),
        name="state_step",
    )(
        branch_in,
        state_real,
        state_imag,
        decay_rate,
        frequency,
        log_step.reshape(1, 64),
        in_re,
        in_im,
        out_re,
        out_im,
        skip_gain.reshape(1, 1024),
    )


def torus_add(me, off):
    core = lax.rem(me + off, 2)
    x = lax.rem(me // 2 + off // 2, 4)
    y = lax.rem(me // 8 + off // 8, 4)
    z = lax.rem(me // 32 + off // 32, 4)
    return ((z * 4 + y) * 4 + x) * 2 + core


def torus_sub(me, off):
    core = lax.rem(me + off, 2)
    x = lax.rem(me // 2 + 4 - lax.rem(off // 2, 4), 4)
    y = lax.rem(me // 8 + 4 - lax.rem(off // 8, 4), 4)
    z = lax.rem(me // 32 + 4 - off // 32, 4)
    return ((z * 4 + y) * 4 + x) * 2 + core


def offset_of(position):
    return lax.rem(position * STRIDE, N_DEV)


def inv_rms(v):
    return lax.rsqrt(jnp.mean(v * v, axis=-1, keepdims=True) + EPS)


def expert_kernel(
    act_ref,
    resid_ref,
    mix_gain_ref,
    in_gain_ref,
    out_gain_ref,
    routes_ref,
    weights_ref,
    glu_value_hbm,
    glu_gate_hbm,
    e_gate_hbm,
    e_up_hbm,
    e_down_hbm,
    s_gate_hbm,
    s_up_hbm,
    s_down_hbm,
    out_ref,
    glu_value,
    glu_gate,
    e_gate,
    e_up,
    e_down,
    s_gate,
    s_up,
    s_down,
    branch,
    resid_mid,
    normed,
    pick,
    weight_hi,
    weight_lo,
    total,
    outgoing,
    received,
    produced,
    returned,
    load_sem,
    send_sem,
    recv_sem,
    back_send_sem,
    back_recv_sem,
):
    me = lax.axis_index("ep")
    barrier = pltpu.get_barrier_semaphore()

    def greet(i, carry):
        pl.semaphore_signal(
            barrier, inc=1, device_id=(lax.rem(me + i, N_DEV),), device_id_type=MESH
        )
        return carry

    lax.fori_loop(1, N_DEV, greet, 0)

    loads = []

    def load(src, dst):
        copy = pltpu.make_async_copy(src, dst, load_sem.at[len(loads)])
        copy.start()
        loads.append(copy)
        return copy

    glu_loads = []
    for n in range(4):
        cols = pl.ds(n * 512, 512)
        glu_loads.append(
            (
                load(glu_value_hbm.at[:, cols], glu_value.at[:, cols]),
                load(glu_gate_hbm.at[:, cols], glu_gate.at[:, cols]),
            )
        )
    s_loads = [load(s_gate_hbm, s_gate), load(s_up_hbm, s_up), load(s_down_hbm, s_down)]
    e_loads = [load(e_gate_hbm, e_gate), load(e_up_hbm, e_up), load(e_down_hbm, e_down)]

    routes = routes_ref[...]
    rel = (
        jnp.bitwise_and(routes + me, 1)
        + jnp.bitwise_and((routes >> 1) + 4 - lax.rem(me // 2, 4), 3) * 2
        + jnp.bitwise_and((routes >> 3) + 4 - lax.rem(me // 8, 4), 3) * 8
        + jnp.bitwise_and((routes >> 5) + 4 - me // 32, 3) * 32
    )
    position = jnp.bitwise_and(rel * STRIDE_INV, N_DEV - 1)
    row = lax.broadcasted_iota(jnp.int32, (SLOTS, 64), 0)
    row_pos = row >> 2
    row_rank = jnp.bitwise_and(row, 3).astype(F32)
    named = jnp.zeros((SLOTS, 64), F32)
    weight = jnp.zeros((SLOTS, 64), F32)
    for k in range(6):
        hit = row_pos == position[k : k + 1, :]
        named = jnp.where(hit, 1.0, named)
        weight = jnp.where(hit, weights_ref[k : k + 1, :], weight)
    earlier = (
        lax.broadcasted_iota(jnp.int32, (64, 64), 0)
        < lax.broadcasted_iota(jnp.int32, (64, 64), 1)
    ).astype(BF16)
    rank = jnp.dot(named.astype(BF16), earlier, preferred_element_type=F32)
    chosen = rank == row_rank
    pick[...] = jnp.where(chosen, named, 0.0).astype(BF16)
    hi, lo = split_hi_lo(jnp.where(chosen, weight, 0.0))
    weight_hi[...] = hi
    weight_lo[...] = lo

    act = act_ref[...]
    square = jnp.zeros((64, 1), F32)
    for n in range(4):
        cols = slice(n * 512, n * 512 + 512)
        for copy in glu_loads[n]:
            copy.wait()
        value_part = jnp.dot(act, glu_value[:, cols], preferred_element_type=F32)
        gate_part = jnp.dot(act, glu_gate[:, cols], preferred_element_type=F32)
        part = value_part * jax.nn.sigmoid(gate_part)
        branch[:, cols] = part
        square = square + jnp.sum(part * part, axis=-1, keepdims=True)
    scale = lax.rsqrt(square * (1.0 / 2048) + EPS)
    mid = (
        resid_ref[...].astype(F32) + branch[...] * scale * mix_gain_ref[...]
    ).astype(BF16)
    resid_mid[...] = mid
    mid = mid.astype(F32)
    normed[...] = (mid * inv_rms(mid) * in_gain_ref[...]).astype(BF16)

    for n in range(4):
        cols = slice(n * 512, n * 512 + 512)
        outgoing[:, cols] = jnp.dot(
            pick[...], normed[:, cols], preferred_element_type=F32
        ).astype(BF16)
    pl.semaphore_wait(barrier, N_DEV - 1)

    def slot(i):
        return pl.ds(pl.multiple_of(i * CAP, CAP), CAP)

    pltpu.make_async_copy(
        outgoing.at[slot(0), :], received.at[slot(0), :], recv_sem.at[0]
    ).start()

    def send(i, carry):
        pltpu.make_async_remote_copy(
            src_ref=outgoing.at[slot(i), :],
            dst_ref=received.at[slot(i), :],
            send_sem=send_sem,
            recv_sem=recv_sem.at[i // GROUP_DEV],
            device_id=(torus_add(me, offset_of(i)),),
            device_id_type=MESH,
        ).start()
        return carry

    lax.fori_loop(1, N_DEV, send, 0)

    for copy in s_loads:
        copy.wait()
    x = normed[...]
    g = jnp.dot(x, s_gate[...], preferred_element_type=F32)
    u = jnp.dot(x, s_up[...], preferred_element_type=F32)
    hidden = (jax.nn.silu(g) * u).astype(BF16)
    for n in range(4):
        cols = slice(n * 512, n * 512 + 512)
        total[:, cols] = jnp.dot(hidden, s_down[:, cols], preferred_element_type=F32)
    for copy in e_loads:
        copy.wait()

    def wait_group(buffer, sem, first, rows):
        part = buffer.at[pl.ds(first, rows), :]
        pltpu.make_async_copy(part, part, sem).wait()

    def back(i, carry):
        pltpu.make_async_remote_copy(
            src_ref=produced.at[slot(i), :],
            dst_ref=returned.at[slot(i), :],
            send_sem=back_send_sem,
            recv_sem=back_recv_sem.at[i // GROUP_DEV],
            device_id=(torus_sub(me, offset_of(i)),),
            device_id_type=MESH,
        ).start()
        return carry

    def run_group(first):
        rows = pl.ds(first, GROUP_ROWS)
        x = received[rows, :]
        g = jnp.dot(x, e_gate[...], preferred_element_type=F32)
        u = jnp.dot(x, e_up[...], preferred_element_type=F32)
        hidden = (jax.nn.silu(g) * u).astype(BF16)
        for n in range(4):
            cols = slice(n * 512, n * 512 + 512)
            produced[rows, cols] = jnp.dot(
                hidden, e_down[:, cols], preferred_element_type=F32
            ).astype(BF16)

    wait_group(received, recv_sem.at[0], 0, GROUP_ROWS)
    run_group(0)
    pltpu.make_async_copy(
        produced.at[slot(0), :], returned.at[slot(0), :], back_recv_sem.at[0]
    ).start()
    lax.fori_loop(1, GROUP_DEV, back, 0)

    def one_group(g, carry):
        first = pl.multiple_of(g * GROUP_ROWS, GROUP_ROWS)
        wait_group(received, recv_sem.at[g], first, GROUP_ROWS)
        run_group(first)
        lax.fori_loop(g * GROUP_DEV, (g + 1) * GROUP_DEV, back, 0)
        return carry

    lax.fori_loop(1, GROUPS, one_group, 0)

    def add_group(first):
        rows = pl.ds(first, GROUP_ROWS)
        left = jnp.concatenate([weight_hi[rows, :], weight_lo[rows, :]], axis=1)
        for n in range(4):
            cols = slice(n * 512, n * 512 + 512)
            both = lax.dot_general(
                left, returned[rows, cols], TN, preferred_element_type=F32
            )
            total[:, cols] += both[:64] + both[64:]

    wait_group(returned, back_recv_sem.at[0], 0, GROUP_ROWS)
    add_group(0)

    def add_one(g, carry):
        first = pl.multiple_of(g * GROUP_ROWS, GROUP_ROWS)
        wait_group(returned, back_recv_sem.at[g], first, GROUP_ROWS)
        add_group(first)
        return carry

    lax.fori_loop(1, GROUPS, add_one, 0)

    combined = total[...]
    out_ref[...] = (
        resid_mid[...].astype(F32)
        + combined * inv_rms(combined) * out_gain_ref[...]
    ).astype(BF16)
    wait_group(s_gate, send_sem, 0, (SLOTS - CAP) * 4)
    wait_group(s_gate, back_send_sem, 0, (SLOTS - CAP) * 4)


def experts(
    activated,
    residual,
    mix_gain,
    moe_in_gain,
    moe_out_gain,
    routes,
    route_weights,
    weights,
):
    vmem = pl.BlockSpec(memory_space=pltpu.VMEM)
    hbm = pl.BlockSpec(memory_space=pl.ANY)
    return pl.pallas_call(
        expert_kernel,
        out_shape=jax.ShapeDtypeStruct((64, 2048), BF16),
        in_specs=[vmem] * 7 + [hbm] * 8,
        out_specs=vmem,
        scratch_shapes=[
            pltpu.VMEM((1024, 2048), BF16),
            pltpu.VMEM((1024, 2048), BF16),
            pltpu.VMEM((2048, 512), BF16),
            pltpu.VMEM((2048, 512), BF16),
            pltpu.VMEM((512, 2048), BF16),
            pltpu.VMEM((2048, 512), BF16),
            pltpu.VMEM((2048, 512), BF16),
            pltpu.VMEM((512, 2048), BF16),
            pltpu.VMEM((64, 2048), F32),
            pltpu.VMEM((64, 2048), BF16),
            pltpu.VMEM((64, 2048), BF16),
            pltpu.VMEM((SLOTS, 64), BF16),
            pltpu.VMEM((SLOTS, 64), BF16),
            pltpu.VMEM((SLOTS, 64), BF16),
            pltpu.VMEM((64, 2048), F32),
            pltpu.VMEM((SLOTS, 2048), BF16),
            pltpu.VMEM((SLOTS, 2048), BF16),
            pltpu.VMEM((SLOTS, 2048), BF16),
            pltpu.VMEM((SLOTS, 2048), BF16),
            pltpu.SemaphoreType.DMA((14,)),
            pltpu.SemaphoreType.DMA,
            pltpu.SemaphoreType.DMA((GROUPS,)),
            pltpu.SemaphoreType.DMA,
            pltpu.SemaphoreType.DMA((GROUPS,)),
        ],
        compiler_params=pltpu.CompilerParams(
            collective_id=0, has_side_effects=True, vmem_limit_bytes=52 * 2**20
        ),
        name="experts",
    )(
        activated,
        residual,
        mix_gain.reshape(1, 2048),
        moe_in_gain.reshape(1, 2048),
        moe_out_gain.reshape(1, 2048),
        jnp.transpose(routes),
        jnp.transpose(route_weights),
        *weights,
    )


def per_device(
    residual,
    branch_in,
    state_real,
    state_imag,
    decay_rate,
    frequency,
    log_step,
    input_real,
    input_imag,
    output_matrix_real,
    output_matrix_imaginary,
    skip_gain,
    glu_value,
    glu_gate,
    mix_gain,
    moe_in_gain,
    moe_out_gain,
    routes,
    route_weights,
    expert_gate,
    expert_up,
    expert_down,
    shared_gate,
    shared_up,
    shared_down,
):
    next_real, next_imag, activated = state_step(
        branch_in,
        state_real,
        state_imag,
        decay_rate,
        frequency,
        log_step,
        input_real,
        input_imag,
        output_matrix_real,
        output_matrix_imaginary,
        skip_gain,
    )
    layer_out = experts(
        activated,
        residual,
        mix_gain,
        moe_in_gain,
        moe_out_gain,
        routes,
        route_weights,
        (
            glu_value,
            glu_gate,
            expert_gate.reshape(2048, 512),
            expert_up.reshape(2048, 512),
            expert_down.reshape(512, 2048),
            shared_gate,
            shared_up,
            shared_down,
        ),
    )
    return layer_out, next_real, next_imag


def solution(mesh):
    return jax.shard_map(
        per_device,
        mesh=mesh,
        in_specs=(
            P("ep", None),
            P("ep", None),
            P("ep", None),
            P("ep", None),
            P(),
            P(),
            P(),
            P(),
            P(),
            P(),
            P(),
            P(),
            P(),
            P(),
            P(),
            P(),
            P(),
            P("ep", None),
            P("ep", None),
            P("ep", None, None),
            P("ep", None, None),
            P("ep", None, None),
            P(),
            P(),
            P(),
        ),
        out_specs=(P("ep", None), P("ep", None), P("ep", None)),
        check_vma=False,
    )
```

```python
import functools

import jax
import jax.numpy as jnp
from jax import lax
from jax.experimental import pallas as pl
from jax.experimental.pallas import tpu as pltpu
from jax.sharding import PartitionSpec as P

MESH = pl.DeviceIdType.MESH
F32 = jnp.float32
BF16 = jnp.bfloat16
EPS = 1e-06
N_DEV = 128
CAP = 4
SLOTS = N_DEV * CAP


def send_order():
    def length(o):
        return sum(min(d, 4 - d) for d in (o % 4, o // 4 % 4, o // 16))

    order = [0]
    for far in sorted(range(1, 64), key=lambda o: -length(o)):
        x, y, z = far % 4, far // 4 % 4, far // 16
        for a, b, c in ((x, y, z), (y, z, x), (z, x, y)):
            for sign in (1, -1):
                image = (sign * a) % 4 + (sign * b) % 4 * 4 + (sign * c) % 4 * 16
                if image not in order:
                    order.append(image)
    return tuple(2 * o + core for o in order for core in (0, 1))


ORDER = send_order()
GROUPS = 4
GROUP_DEV = N_DEV // GROUPS
GROUP_ROWS = SLOTS // GROUPS
NT = (((1,), (1,)), ((), ()))
TN = (((0,), (0,)), ((), ()))


def keep(value):
    return pltpu.with_memory_space_constraint(value, memory_space=pltpu.HBM)


def ahead(value):
    return pltpu.with_memory_space_constraint(value, memory_space=pltpu.VMEM)


def split_hi_lo(value):
    hi = value.astype(BF16)
    lo = (value - hi.astype(F32)).astype(BF16)
    return hi, lo


SSM_STEPS = 4
BLOCKS_PER_STEP = 8 // SSM_STEPS


def state_kernel(
    feed_ref,
    re_ref,
    im_ref,
    decay_ref,
    freq_ref,
    log_step_ref,
    in_re_ref,
    in_im_ref,
    out_re_ref,
    out_im_ref,
    skip_ref,
    next_re_ref,
    next_im_ref,
    act_ref,
):
    step = pl.program_id(0)
    rows = 8 * BLOCKS_PER_STEP
    group = lax.broadcasted_iota(jnp.int32, (rows, 64), 0) + step * rows
    lane = lax.broadcasted_iota(jnp.int32, (rows, 64), 1)
    column = jnp.sum(
        jnp.where(group == lane, jnp.broadcast_to(log_step_ref[...], (rows, 64)), 0.0),
        axis=1,
        keepdims=True,
    )
    step_size = jnp.exp(column)
    decay = decay_ref[...]
    freq = freq_ref[...]
    magnitude = jnp.exp(-decay * step_size)
    phase = freq * step_size
    abar_re = magnitude * jnp.cos(phase)
    abar_im = magnitude * jnp.sin(phase)
    denominator = decay * decay + freq * freq
    numer_re = abar_re - 1.0
    coef_re = (abar_im * freq - numer_re * decay) / denominator
    coef_im = (-abar_im * decay - numer_re * freq) / denominator

    def twice(v):
        return jnp.concatenate([v, v], axis=1)

    abar_re, abar_im, coef_re, coef_im = map(
        twice, (abar_re, abar_im, coef_re, coef_im)
    )
    row_group = lax.broadcasted_iota(jnp.int32, (128, 128), 0) // 16
    lane_half = lax.broadcasted_iota(jnp.int32, (128, 128), 1) // 64
    low_half = lax.broadcasted_iota(jnp.int32, (1, 128), 1) < 64
    for b in range(BLOCKS_PER_STEP):
        bb_re, bb_im = [], []
        for g in range(8):
            r = b * 8 + g
            own = slice(r * 16, r * 16 + 16)
            b_re = twice(in_re_ref[own, :].astype(F32))
            b_im = twice(in_im_ref[own, :].astype(F32))
            c_re, c_im = coef_re[r : r + 1, :], coef_im[r : r + 1, :]
            bb_re.append(c_re * b_re - c_im * b_im)
            bb_im.append(c_re * b_im + c_im * b_re)
        bb_re = jnp.concatenate(bb_re, axis=0)
        bb_im = jnp.concatenate(bb_im, axis=0)
        rows_here = slice(b * 128, b * 128 + 128)
        o_re = twice(out_re_ref[rows_here, :].astype(F32))
        o_im = twice(-out_im_ref[rows_here, :].astype(F32))
        parts_re_hi, parts_re_lo = split_hi_lo(bb_re)
        parts_im_hi, parts_im_lo = split_hi_lo(bb_im)
        feed = feed_ref[:, b * 128 : b * 128 + 128]
        feed_twice = jnp.concatenate([feed, feed], axis=1)
        readout = jnp.zeros((64, 128), F32)
        for q in range(4):
            mask = row_group == 2 * q + lane_half
            zero = jnp.zeros((128, 128), BF16)

            def block(hi, lo):
                return jnp.concatenate(
                    [jnp.where(mask, hi, zero), jnp.where(mask, lo, zero)], axis=0
                )

            f_re = jnp.dot(
                feed_twice, block(parts_re_hi, parts_re_lo), preferred_element_type=F32
            )
            f_im = jnp.dot(
                feed_twice, block(parts_im_hi, parts_im_lo), preferred_element_type=F32
            )
            r0 = b * 8 + 2 * q
            a_re = jnp.where(
                low_half, abar_re[r0 : r0 + 1, :], abar_re[r0 + 1 : r0 + 2, :]
            )
            a_im = jnp.where(
                low_half, abar_im[r0 : r0 + 1, :], abar_im[r0 + 1 : r0 + 2, :]
            )
            lanes = slice(b * 512 + q * 128, b * 512 + q * 128 + 128)
            old_re, old_im = re_ref[:, lanes], im_ref[:, lanes]
            new_re = a_re * old_re - a_im * old_im + f_re
            new_im = a_re * old_im + a_im * old_re + f_im
            next_re_ref[:, lanes] = new_re
            next_im_ref[:, lanes] = new_im
            re_hi, re_lo = split_hi_lo(new_re)
            im_hi, im_lo = split_hi_lo(new_im)
            w = jnp.concatenate(
                [
                    jnp.where(mask, o_re, 0.0).astype(BF16),
                    jnp.where(mask, o_im, 0.0).astype(BF16),
                ],
                axis=1,
            )
            left = jnp.concatenate(
                [
                    jnp.concatenate([re_hi, im_hi], axis=1),
                    jnp.concatenate([re_lo, im_lo], axis=1),
                ],
                axis=0,
            )
            both = lax.dot_general(left, w, NT, preferred_element_type=F32)
            readout = readout + (both[:64] + both[64:])
        here = slice(b * 128, b * 128 + 128)
        mixed = readout + skip_ref[:, here] * feed.astype(F32)
        act_ref[:, here] = jax.nn.gelu(mixed).astype(BF16)


def state_step(
    branch_in,
    state_real,
    state_imag,
    decay_rate,
    frequency,
    log_step,
    input_real,
    input_imag,
    output_matrix_real,
    output_matrix_imaginary,
    skip_gain,
):
    in_re = jnp.transpose(input_real, (0, 2, 1)).reshape(1024, 64)
    in_im = jnp.transpose(input_imag, (0, 2, 1)).reshape(1024, 64)
    out_re = output_matrix_real.reshape(1024, 64)
    out_im = output_matrix_imaginary.reshape(1024, 64)
    n = SSM_STEPS
    wide = pl.BlockSpec((64, 4096 // n), lambda i: (0, i))
    narrow = pl.BlockSpec((64, 1024 // n), lambda i: (0, i))
    per_group = pl.BlockSpec((64 // n, 64), lambda i: (i, 0))
    per_channel = pl.BlockSpec((1024 // n, 64), lambda i: (i, 0))
    return pl.pallas_call(
        state_kernel,
        grid=(n,),
        out_shape=(
            jax.ShapeDtypeStruct((64, 4096), F32),
            jax.ShapeDtypeStruct((64, 4096), F32),
            jax.ShapeDtypeStruct((64, 1024), BF16),
        ),
        in_specs=[
            narrow,
            wide,
            wide,
            per_group,
            per_group,
            pl.BlockSpec((1, 64), lambda i: (0, 0)),
            per_channel,
            per_channel,
            per_channel,
            per_channel,
            pl.BlockSpec((1, 1024 // n), lambda i: (0, i)),
        ],
        out_specs=(wide, wide, narrow),
        compiler_params=pltpu.CompilerParams(
            dimension_semantics=("arbitrary",), vmem_limit_bytes=20 * 2**20
        ),
        cost_estimate=pl.CostEstimate(
            flops=4_000_000_000, bytes_accessed=6_000_000, transcendentals=100_000
        ),
        name="state_step",
    )(
        keep(branch_in),
        keep(state_real),
        keep(state_imag),
        keep(decay_rate),
        keep(frequency),
        keep(log_step.reshape(1, 64)),
        keep(in_re),
        keep(in_im),
        keep(out_re),
        keep(out_im),
        keep(skip_gain.reshape(1, 1024)),
    )


def torus_add(me, off):
    core = lax.rem(me + off, 2)
    x = lax.rem(me // 2 + off // 2, 4)
    y = lax.rem(me // 8 + off // 8, 4)
    z = lax.rem(me // 32 + off // 32, 4)
    return ((z * 4 + y) * 4 + x) * 2 + core


def torus_sub(me, off):
    core = lax.rem(me + off, 2)
    x = lax.rem(me // 2 + 4 - lax.rem(off // 2, 4), 4)
    y = lax.rem(me // 8 + 4 - lax.rem(off // 8, 4), 4)
    z = lax.rem(me // 32 + 4 - off // 32, 4)
    return ((z * 4 + y) * 4 + x) * 2 + core


def inv_rms(v):
    return lax.rsqrt(jnp.mean(v * v, axis=-1, keepdims=True) + EPS)


def expert_kernel(
    act_ref,
    resid_ref,
    mix_gain_ref,
    in_gain_ref,
    out_gain_ref,
    routes_ref,
    weights_ref,
    glu_value,
    glu_gate,
    e_gate_hbm,
    e_up_hbm,
    e_down_hbm,
    s_gate_hbm,
    s_up_hbm,
    s_down_hbm,
    out_ref,
    e_gate,
    e_up,
    e_down,
    s_gate,
    s_up,
    s_down,
    branch,
    resid_mid,
    normed,
    pick,
    weight_hi,
    weight_lo,
    total,
    outgoing,
    received,
    produced,
    returned,
    load_sem,
    send_sem,
    recv_sem,
    back_send_sem,
    back_recv_sem,
    plane_sem,
    all_sem,
):
    me = lax.axis_index("ep")
    barrier = pltpu.get_barrier_semaphore()

    line_x = [torus_add(me, o) for o in range(1, 8)]
    line_y = [torus_add(me, 8 * o) for o in range(1, 4)]
    line_z = [torus_add(me, 32 * o) for o in range(1, 4)]

    def greet(sem, devices):
        for device in devices:
            pl.semaphore_signal(
                sem, inc=1, device_id=(device,), device_id_type=MESH
            )

    greet(barrier, line_x + line_y + line_z)

    loads = []

    def load(src, dst):
        copy = pltpu.make_async_copy(src, dst, load_sem.at[len(loads)])
        copy.start()
        loads.append(copy)
        return copy

    s_loads = [load(s_gate_hbm, s_gate), load(s_up_hbm, s_up), load(s_down_hbm, s_down)]
    e_loads = [load(e_gate_hbm, e_gate), load(e_up_hbm, e_up), load(e_down_hbm, e_down)]

    routes = routes_ref[...]
    rel = (
        jnp.bitwise_and(routes + me, 1)
        + jnp.bitwise_and((routes >> 1) + 4 - lax.rem(me // 2, 4), 3) * 2
        + jnp.bitwise_and((routes >> 3) + 4 - lax.rem(me // 8, 4), 3) * 8
        + jnp.bitwise_and((routes >> 5) + 4 - me // 32, 3) * 32
    )
    position = jnp.zeros_like(rel)
    for i in range(1, N_DEV):
        position = jnp.where(rel == ORDER[i], i, position)
    row = lax.broadcasted_iota(jnp.int32, (SLOTS, 64), 0)
    row_pos = row >> 2
    row_rank = jnp.bitwise_and(row, 3).astype(F32)
    named = jnp.zeros((SLOTS, 64), F32)
    weight = jnp.zeros((SLOTS, 64), F32)
    for k in range(6):
        hit = row_pos == position[k : k + 1, :]
        named = jnp.where(hit, 1.0, named)
        weight = jnp.where(hit, weights_ref[k : k + 1, :], weight)
    earlier = (
        lax.broadcasted_iota(jnp.int32, (64, 64), 0)
        < lax.broadcasted_iota(jnp.int32, (64, 64), 1)
    ).astype(BF16)
    rank = jnp.dot(named.astype(BF16), earlier, preferred_element_type=F32)
    chosen = rank == row_rank
    pick[...] = jnp.where(chosen, named, 0.0).astype(BF16)
    hi, lo = split_hi_lo(jnp.where(chosen, weight, 0.0))
    weight_hi[...] = hi
    weight_lo[...] = lo

    pl.semaphore_wait(barrier, 13)
    greet(plane_sem, line_y)

    act = act_ref[...]
    square = jnp.zeros((64, 1), F32)
    for n in range(4):
        cols = slice(n * 512, n * 512 + 512)
        value_part = jnp.dot(act, glu_value[:, cols], preferred_element_type=F32)
        gate_part = jnp.dot(act, glu_gate[:, cols], preferred_element_type=F32)
        part = value_part * jax.nn.sigmoid(gate_part)
        branch[:, cols] = part
        square = square + jnp.sum(part * part, axis=-1, keepdims=True)
        if n == 1:
            pl.semaphore_wait(plane_sem, 3)
            greet(all_sem, line_z)
    scale = lax.rsqrt(square * (1.0 / 2048) + EPS)
    mid = (
        resid_ref[...].astype(F32) + branch[...] * scale * mix_gain_ref[...]
    ).astype(BF16)
    resid_mid[...] = mid
    mid = mid.astype(F32)
    normed[...] = (mid * inv_rms(mid) * in_gain_ref[...]).astype(BF16)

    for n in range(4):
        cols = slice(n * 512, n * 512 + 512)
        outgoing[:, cols] = jnp.dot(
            pick[...], normed[:, cols], preferred_element_type=F32
        ).astype(BF16)
    pl.semaphore_wait(all_sem, 3)

    def slot(i):
        return pl.ds(i * CAP, CAP)

    pltpu.make_async_copy(
        outgoing.at[slot(0), :], received.at[slot(0), :], recv_sem.at[0]
    ).start()

    for i in range(1, N_DEV):
        pltpu.make_async_remote_copy(
            src_ref=outgoing.at[slot(i), :],
            dst_ref=received.at[slot(i), :],
            send_sem=send_sem,
            recv_sem=recv_sem.at[i // GROUP_DEV],
            device_id=(torus_add(me, ORDER[i]),),
            device_id_type=MESH,
        ).start()

    for copy in s_loads:
        copy.wait()
    x = normed[...]
    g = jnp.dot(x, s_gate[...], preferred_element_type=F32)
    u = jnp.dot(x, s_up[...], preferred_element_type=F32)
    hidden = (jax.nn.silu(g) * u).astype(BF16)
    for n in range(4):
        cols = slice(n * 512, n * 512 + 512)
        total[:, cols] = jnp.dot(hidden, s_down[:, cols], preferred_element_type=F32)
    for copy in e_loads:
        copy.wait()

    def wait_group(buffer, sem, first, rows):
        part = buffer.at[pl.ds(first, rows), :]
        pltpu.make_async_copy(part, part, sem).wait()

    def back(i):
        pltpu.make_async_remote_copy(
            src_ref=produced.at[slot(i), :],
            dst_ref=returned.at[slot(i), :],
            send_sem=back_send_sem,
            recv_sem=back_recv_sem.at[i // GROUP_DEV],
            device_id=(torus_sub(me, ORDER[i]),),
            device_id_type=MESH,
        ).start()

    def run_group(first):
        rows = pl.ds(first, GROUP_ROWS)
        x = received[rows, :]
        g = jnp.dot(x, e_gate[...], preferred_element_type=F32)
        u = jnp.dot(x, e_up[...], preferred_element_type=F32)
        hidden = (jax.nn.silu(g) * u).astype(BF16)
        for n in range(4):
            cols = slice(n * 512, n * 512 + 512)
            produced[rows, cols] = jnp.dot(
                hidden, e_down[:, cols], preferred_element_type=F32
            ).astype(BF16)

    for g in range(GROUPS):
        wait_group(received, recv_sem.at[g], g * GROUP_ROWS, GROUP_ROWS)
        run_group(g * GROUP_ROWS)
        for i in range(g * GROUP_DEV, (g + 1) * GROUP_DEV):
            if i == 0:
                pltpu.make_async_copy(
                    produced.at[slot(0), :], returned.at[slot(0), :], back_recv_sem.at[0]
                ).start()
            else:
                back(i)

    def add_group(first):
        rows = pl.ds(first, GROUP_ROWS)
        left = jnp.concatenate([weight_hi[rows, :], weight_lo[rows, :]], axis=1)
        for n in range(4):
            cols = slice(n * 512, n * 512 + 512)
            both = lax.dot_general(
                left, returned[rows, cols], TN, preferred_element_type=F32
            )
            total[:, cols] += both[:64] + both[64:]

    wait_group(returned, back_recv_sem.at[0], 0, GROUP_ROWS)
    add_group(0)

    def add_one(g, carry):
        first = pl.multiple_of(g * GROUP_ROWS, GROUP_ROWS)
        wait_group(returned, back_recv_sem.at[g], first, GROUP_ROWS)
        add_group(first)
        return carry

    lax.fori_loop(1, GROUPS, add_one, 0)

    combined = total[...]
    out_ref[...] = (
        resid_mid[...].astype(F32)
        + combined * inv_rms(combined) * out_gain_ref[...]
    ).astype(BF16)
    wait_group(s_gate, send_sem, 0, (SLOTS - CAP) * 4)
    wait_group(s_gate, back_send_sem, 0, (SLOTS - CAP) * 4)


def experts(
    activated,
    residual,
    mix_gain,
    moe_in_gain,
    moe_out_gain,
    routes,
    route_weights,
    weights,
):
    vmem = pl.BlockSpec(memory_space=pltpu.VMEM)
    hbm = pl.BlockSpec(memory_space=pl.ANY)
    return pl.pallas_call(
        expert_kernel,
        out_shape=jax.ShapeDtypeStruct((64, 2048), BF16),
        in_specs=[vmem] * 9 + [hbm] * 6,
        out_specs=vmem,
        scratch_shapes=[
            pltpu.VMEM((2048, 512), BF16),
            pltpu.VMEM((2048, 512), BF16),
            pltpu.VMEM((512, 2048), BF16),
            pltpu.VMEM((2048, 512), BF16),
            pltpu.VMEM((2048, 512), BF16),
            pltpu.VMEM((512, 2048), BF16),
            pltpu.VMEM((64, 2048), F32),
            pltpu.VMEM((64, 2048), BF16),
            pltpu.VMEM((64, 2048), BF16),
            pltpu.VMEM((SLOTS, 64), BF16),
            pltpu.VMEM((SLOTS, 64), BF16),
            pltpu.VMEM((SLOTS, 64), BF16),
            pltpu.VMEM((64, 2048), F32),
            pltpu.VMEM((SLOTS, 2048), BF16),
            pltpu.VMEM((SLOTS, 2048), BF16),
            pltpu.VMEM((SLOTS, 2048), BF16),
            pltpu.VMEM((SLOTS, 2048), BF16),
            pltpu.SemaphoreType.DMA((14,)),
            pltpu.SemaphoreType.DMA,
            pltpu.SemaphoreType.DMA((GROUPS,)),
            pltpu.SemaphoreType.DMA,
            pltpu.SemaphoreType.DMA((GROUPS,)),
            pltpu.SemaphoreType.REGULAR,
            pltpu.SemaphoreType.REGULAR,
        ],
        compiler_params=pltpu.CompilerParams(
            collective_id=0, has_side_effects=True, vmem_limit_bytes=40 * 2**20
        ),
        name="experts",
    )(
        activated,
        residual,
        mix_gain.reshape(1, 2048),
        moe_in_gain.reshape(1, 2048),
        moe_out_gain.reshape(1, 2048),
        jnp.transpose(routes),
        jnp.transpose(route_weights),
        ahead(weights[0]),
        ahead(weights[1]),
        *map(keep, weights[2:]),
    )


def per_device(
    residual,
    branch_in,
    state_real,
    state_imag,
    decay_rate,
    frequency,
    log_step,
    input_real,
    input_imag,
    output_matrix_real,
    output_matrix_imaginary,
    skip_gain,
    glu_value,
    glu_gate,
    mix_gain,
    moe_in_gain,
    moe_out_gain,
    routes,
    route_weights,
    expert_gate,
    expert_up,
    expert_down,
    shared_gate,
    shared_up,
    shared_down,
):
    next_real, next_imag, activated = state_step(
        branch_in,
        state_real,
        state_imag,
        decay_rate,
        frequency,
        log_step,
        input_real,
        input_imag,
        output_matrix_real,
        output_matrix_imaginary,
        skip_gain,
    )
    layer_out = experts(
        activated,
        residual,
        mix_gain,
        moe_in_gain,
        moe_out_gain,
        routes,
        route_weights,
        (
            glu_value,
            glu_gate,
            expert_gate.reshape(2048, 512),
            expert_up.reshape(2048, 512),
            expert_down.reshape(512, 2048),
            shared_gate,
            shared_up,
            shared_down,
        ),
    )
    return layer_out, next_real, next_imag


def solution(mesh):
    return jax.shard_map(
        per_device,
        mesh=mesh,
        in_specs=(
            P("ep", None),
            P("ep", None),
            P("ep", None),
            P("ep", None),
            P(),
            P(),
            P(),
            P(),
            P(),
            P(),
            P(),
            P(),
            P(),
            P(),
            P(),
            P(),
            P(),
            P("ep", None),
            P("ep", None),
            P("ep", None, None),
            P("ep", None, None),
            P("ep", None, None),
            P(),
            P(),
            P(),
        ),
        out_specs=(P("ep", None), P("ep", None), P("ep", None)),
        check_vma=False,
    )
```

```python
import functools

import jax
import jax.numpy as jnp
from jax import lax
from jax.experimental import pallas as pl
from jax.experimental.pallas import tpu as pltpu
from jax.sharding import PartitionSpec as P

MESH = pl.DeviceIdType.MESH
F32 = jnp.float32
BF16 = jnp.bfloat16
EPS = 1e-06
N_DEV = 128
CAP = 4
SLOTS = N_DEV * CAP


def send_order():
    def length(o):
        return sum(min(d, 4 - d) for d in (o % 4, o // 4 % 4, o // 16))

    order = [0]
    for far in sorted(range(1, 64), key=lambda o: -length(o)):
        x, y, z = far % 4, far // 4 % 4, far // 16
        for a, b, c in ((x, y, z), (y, z, x), (z, x, y)):
            for sign in (1, -1):
                image = (sign * a) % 4 + (sign * b) % 4 * 4 + (sign * c) % 4 * 16
                if image not in order:
                    order.append(image)
    return tuple(2 * o + core for o in order for core in (0, 1))


ORDER = send_order()
GROUPS = 4
GROUP_DEV = N_DEV // GROUPS
GROUP_ROWS = SLOTS // GROUPS
NT = (((1,), (1,)), ((), ()))
TN = (((0,), (0,)), ((), ()))


def keep(value):
    return pltpu.with_memory_space_constraint(value, memory_space=pltpu.HBM)


def split_hi_lo(value):
    hi = value.astype(BF16)
    lo = (value - hi.astype(F32)).astype(BF16)
    return hi, lo


def twice(v):
    return jnp.concatenate([v, v], axis=1)


def state_constants(decay, freq, log_step):
    group = lax.broadcasted_iota(jnp.int32, (64, 64), 0)
    lane = lax.broadcasted_iota(jnp.int32, (64, 64), 1)
    column = jnp.sum(
        jnp.where(group == lane, jnp.broadcast_to(log_step, (64, 64)), 0.0),
        axis=1,
        keepdims=True,
    )
    step_size = jnp.exp(column)
    magnitude = jnp.exp(-decay * step_size)
    phase = freq * step_size
    abar_re = magnitude * jnp.cos(phase)
    abar_im = magnitude * jnp.sin(phase)
    denominator = decay * decay + freq * freq
    numer_re = abar_re - 1.0
    coef_re = (abar_im * freq - numer_re * decay) / denominator
    coef_im = (-abar_im * decay - numer_re * freq) / denominator
    return tuple(map(twice, (abar_re, abar_im, coef_re, coef_im)))


def state_block(
    b,
    constants,
    feed_ref,
    re_ref,
    im_ref,
    in_re_ref,
    in_im_ref,
    out_re_ref,
    out_im_ref,
    skip_ref,
    next_re_ref,
    next_im_ref,
    act_ref,
):
    abar_re, abar_im, coef_re, coef_im = constants
    row_group = lax.broadcasted_iota(jnp.int32, (128, 128), 0) // 16
    lane_half = lax.broadcasted_iota(jnp.int32, (128, 128), 1) // 64
    low_half = lax.broadcasted_iota(jnp.int32, (1, 128), 1) < 64
    bb_re, bb_im = [], []
    for r in range(b * 8, b * 8 + 8):
        own = slice(r * 16, r * 16 + 16)
        b_re = twice(in_re_ref[own, :].astype(F32))
        b_im = twice(in_im_ref[own, :].astype(F32))
        c_re, c_im = coef_re[r : r + 1, :], coef_im[r : r + 1, :]
        bb_re.append(c_re * b_re - c_im * b_im)
        bb_im.append(c_re * b_im + c_im * b_re)
    here = slice(b * 128, b * 128 + 128)
    o_re = twice(out_re_ref[here, :].astype(F32))
    o_im = twice(-out_im_ref[here, :].astype(F32))
    parts_re_hi, parts_re_lo = split_hi_lo(jnp.concatenate(bb_re, axis=0))
    parts_im_hi, parts_im_lo = split_hi_lo(jnp.concatenate(bb_im, axis=0))
    feed = feed_ref[:, here]
    feed_twice = twice(feed)
    readout = jnp.zeros((64, 128), F32)
    zero = jnp.zeros((128, 128), BF16)
    for q in range(4):
        mask = row_group == 2 * q + lane_half

        def block(hi, lo):
            return jnp.concatenate(
                [jnp.where(mask, hi, zero), jnp.where(mask, lo, zero)], axis=0
            )

        f_re = jnp.dot(
            feed_twice, block(parts_re_hi, parts_re_lo), preferred_element_type=F32
        )
        f_im = jnp.dot(
            feed_twice, block(parts_im_hi, parts_im_lo), preferred_element_type=F32
        )
        r0 = b * 8 + 2 * q
        a_re = jnp.where(low_half, abar_re[r0 : r0 + 1, :], abar_re[r0 + 1 : r0 + 2, :])
        a_im = jnp.where(low_half, abar_im[r0 : r0 + 1, :], abar_im[r0 + 1 : r0 + 2, :])
        lanes = slice(b * 512 + q * 128, b * 512 + q * 128 + 128)
        old_re, old_im = re_ref[:, lanes], im_ref[:, lanes]
        new_re = a_re * old_re - a_im * old_im + f_re
        new_im = a_re * old_im + a_im * old_re + f_im
        next_re_ref[:, lanes] = new_re
        next_im_ref[:, lanes] = new_im
        re_hi, re_lo = split_hi_lo(new_re)
        im_hi, im_lo = split_hi_lo(new_im)
        w = jnp.concatenate(
            [
                jnp.where(mask, o_re, 0.0).astype(BF16),
                jnp.where(mask, o_im, 0.0).astype(BF16),
            ],
            axis=1,
        )
        left = jnp.concatenate(
            [
                jnp.concatenate([re_hi, im_hi], axis=1),
                jnp.concatenate([re_lo, im_lo], axis=1),
            ],
            axis=0,
        )
        both = lax.dot_general(left, w, NT, preferred_element_type=F32)
        readout = readout + (both[:64] + both[64:])
    mixed = readout + skip_ref[:, here] * feed.astype(F32)
    act_ref[:, here] = jax.nn.gelu(mixed).astype(BF16)


def torus_add(me, off):
    core = lax.rem(me + off, 2)
    x = lax.rem(me // 2 + off // 2, 4)
    y = lax.rem(me // 8 + off // 8, 4)
    z = lax.rem(me // 32 + off // 32, 4)
    return ((z * 4 + y) * 4 + x) * 2 + core


def torus_sub(me, off):
    core = lax.rem(me + off, 2)
    x = lax.rem(me // 2 + 4 - lax.rem(off // 2, 4), 4)
    y = lax.rem(me // 8 + 4 - lax.rem(off // 8, 4), 4)
    z = lax.rem(me // 32 + 4 - off // 32, 4)
    return ((z * 4 + y) * 4 + x) * 2 + core


def inv_rms(v):
    return lax.rsqrt(jnp.mean(v * v, axis=-1, keepdims=True) + EPS)


SMALL = (
    ("log_step", (1, 64), F32),
    ("decay", (64, 64), F32),
    ("freq", (64, 64), F32),
    ("routes", (6, 64), jnp.int32),
    ("weights", (6, 64), F32),
    ("feed", (64, 1024), BF16),
    ("in_re", (1024, 64), BF16),
    ("in_im", (1024, 64), BF16),
    ("out_re", (1024, 64), BF16),
    ("out_im", (1024, 64), BF16),
    ("skip", (1, 1024), F32),
    ("resid", (64, 2048), BF16),
    ("mix_gain", (1, 2048), F32),
    ("in_gain", (1, 2048), F32),
    ("out_gain", (1, 2048), F32),
)
STATE_PARTS = 4


def layer_kernel(*refs):
    n = len(SMALL)
    small_hbm, refs = refs[:n], refs[n:]
    (
        re_hbm,
        im_hbm,
        glu_value_hbm,
        glu_gate_hbm,
        e_gate_hbm,
        e_up_hbm,
        e_down_hbm,
        s_gate_hbm,
        s_up_hbm,
        s_down_hbm,
        out_ref,
        next_re,
        next_im,
    ) = refs[:13]
    refs = refs[13:]
    small, refs = refs[:n], refs[n:]
    (
        log_step_ref,
        decay_ref,
        freq_ref,
        routes_ref,
        weights_ref,
        feed_ref,
        in_re_ref,
        in_im_ref,
        out_re_ref,
        out_im_ref,
        skip_ref,
        resid_ref,
        mix_gain_ref,
        in_gain_ref,
        out_gain_ref,
    ) = small
    (
        old_re,
        old_im,
        act_ref,
        glu_value,
        glu_gate,
        e_gate,
        e_up,
        e_down,
        s_gate,
        s_up,
        s_down,
        branch,
        resid_mid,
        normed,
        pick,
        weight_hi,
        weight_lo,
        total,
        outgoing,
        received,
        produced,
        returned,
        load_sem,
        send_sem,
        recv_sem,
        back_send_sem,
        back_recv_sem,
        plane_sem,
        all_sem,
    ) = refs
    me = lax.axis_index("ep")
    barrier = pltpu.get_barrier_semaphore()

    line_x = [torus_add(me, o) for o in range(1, 8)]
    line_y = [torus_add(me, 8 * o) for o in range(1, 4)]
    line_z = [torus_add(me, 32 * o) for o in range(1, 4)]

    def greet(sem, devices):
        for device in devices:
            pl.semaphore_signal(
                sem, inc=1, device_id=(device,), device_id_type=MESH
            )

    greet(barrier, line_x + line_y + line_z)

    loads = []

    def load(src, dst):
        copy = pltpu.make_async_copy(src, dst, load_sem.at[len(loads)])
        copy.start()
        loads.append(copy)
        return copy

    small_loads = [load(src, dst) for src, dst in zip(small_hbm, small)]
    state_loads = []
    for part in range(STATE_PARTS):
        cols = pl.ds(part * 4096 // STATE_PARTS, 4096 // STATE_PARTS)
        state_loads.append(
            (
                load(re_hbm.at[:, cols], old_re.at[:, cols]),
                load(im_hbm.at[:, cols], old_im.at[:, cols]),
            )
        )
    glu_loads = []
    for part in range(4):
        cols = pl.ds(part * 512, 512)
        glu_loads.append(
            (
                load(glu_value_hbm.at[:, cols], glu_value.at[:, cols]),
                load(glu_gate_hbm.at[:, cols], glu_gate.at[:, cols]),
            )
        )
    for copy in small_loads[:5]:
        copy.wait()
    constants = state_constants(decay_ref[...], freq_ref[...], log_step_ref[...])

    routes = routes_ref[...]
    rel = (
        jnp.bitwise_and(routes + me, 1)
        + jnp.bitwise_and((routes >> 1) + 4 - lax.rem(me // 2, 4), 3) * 2
        + jnp.bitwise_and((routes >> 3) + 4 - lax.rem(me // 8, 4), 3) * 8
        + jnp.bitwise_and((routes >> 5) + 4 - me // 32, 3) * 32
    )
    position = jnp.zeros_like(rel)
    for i in range(1, N_DEV):
        position = jnp.where(rel == ORDER[i], i, position)
    row = lax.broadcasted_iota(jnp.int32, (SLOTS, 64), 0)
    row_pos = row >> 2
    row_rank = jnp.bitwise_and(row, 3).astype(F32)
    named = jnp.zeros((SLOTS, 64), F32)
    weight = jnp.zeros((SLOTS, 64), F32)
    for k in range(6):
        hit = row_pos == position[k : k + 1, :]
        named = jnp.where(hit, 1.0, named)
        weight = jnp.where(hit, weights_ref[k : k + 1, :], weight)
    earlier = (
        lax.broadcasted_iota(jnp.int32, (64, 64), 0)
        < lax.broadcasted_iota(jnp.int32, (64, 64), 1)
    ).astype(BF16)
    rank = jnp.dot(named.astype(BF16), earlier, preferred_element_type=F32)
    chosen = rank == row_rank
    pick[...] = jnp.where(chosen, named, 0.0).astype(BF16)
    hi, lo = split_hi_lo(jnp.where(chosen, weight, 0.0))
    weight_hi[...] = hi
    weight_lo[...] = lo

    for copy in small_loads[5:]:
        copy.wait()
    for part in range(STATE_PARTS):
        for copy in state_loads[part]:
            copy.wait()
        for b in range(part * 8 // STATE_PARTS, (part + 1) * 8 // STATE_PARTS):
            state_block(
                b,
                constants,
                feed_ref,
                old_re,
                old_im,
                in_re_ref,
                in_im_ref,
                out_re_ref,
                out_im_ref,
                skip_ref,
                next_re,
                next_im,
                act_ref,
            )
        if part == 1:
            pl.semaphore_wait(barrier, 13)
            greet(plane_sem, line_y)
    pl.semaphore_wait(plane_sem, 3)
    greet(all_sem, line_z)
    s_loads = [load(s_gate_hbm, s_gate), load(s_up_hbm, s_up), load(s_down_hbm, s_down)]
    e_loads = [load(e_gate_hbm, e_gate), load(e_up_hbm, e_up), load(e_down_hbm, e_down)]

    act = act_ref[...]
    square = jnp.zeros((64, 1), F32)
    for n in range(4):
        cols = slice(n * 512, n * 512 + 512)
        for copy in glu_loads[n]:
            copy.wait()
        value_part = jnp.dot(act, glu_value[:, cols], preferred_element_type=F32)
        gate_part = jnp.dot(act, glu_gate[:, cols], preferred_element_type=F32)
        part = value_part * jax.nn.sigmoid(gate_part)
        branch[:, cols] = part
        square = square + jnp.sum(part * part, axis=-1, keepdims=True)
    scale = lax.rsqrt(square * (1.0 / 2048) + EPS)
    mid = (
        resid_ref[...].astype(F32) + branch[...] * scale * mix_gain_ref[...]
    ).astype(BF16)
    resid_mid[...] = mid
    mid = mid.astype(F32)
    normed[...] = (mid * inv_rms(mid) * in_gain_ref[...]).astype(BF16)

    def slot(i):
        return pl.ds(i * CAP, CAP)

    for g in range(GROUPS):
        rows = slice(g * GROUP_ROWS, (g + 1) * GROUP_ROWS)
        outgoing[rows, :] = jnp.dot(
            pick[rows, :], normed[...], preferred_element_type=F32
        ).astype(BF16)
        if g == 0:
            pl.semaphore_wait(all_sem, 3)
            pltpu.make_async_copy(
                outgoing.at[slot(0), :], received.at[slot(0), :], recv_sem.at[0]
            ).start()
        for i in range(max(1, g * GROUP_DEV), (g + 1) * GROUP_DEV):
            pltpu.make_async_remote_copy(
                src_ref=outgoing.at[slot(i), :],
                dst_ref=received.at[slot(i), :],
                send_sem=send_sem,
                recv_sem=recv_sem.at[g],
                device_id=(torus_add(me, ORDER[i]),),
                device_id_type=MESH,
            ).start()

    for copy in s_loads:
        copy.wait()
    x = normed[...]
    g = jnp.dot(x, s_gate[...], preferred_element_type=F32)
    u = jnp.dot(x, s_up[...], preferred_element_type=F32)
    hidden = (jax.nn.silu(g) * u).astype(BF16)
    for n in range(4):
        cols = slice(n * 512, n * 512 + 512)
        total[:, cols] = jnp.dot(hidden, s_down[:, cols], preferred_element_type=F32)
    for copy in e_loads:
        copy.wait()

    def wait_group(buffer, sem, first, rows):
        part = buffer.at[pl.ds(first, rows), :]
        pltpu.make_async_copy(part, part, sem).wait()

    def back(i):
        pltpu.make_async_remote_copy(
            src_ref=produced.at[slot(i), :],
            dst_ref=returned.at[slot(i), :],
            send_sem=back_send_sem,
            recv_sem=back_recv_sem.at[i // GROUP_DEV],
            device_id=(torus_sub(me, ORDER[i]),),
            device_id_type=MESH,
        ).start()

    def run_group(first):
        rows = pl.ds(first, GROUP_ROWS)
        x = received[rows, :]
        g = jnp.dot(x, e_gate[...], preferred_element_type=F32)
        u = jnp.dot(x, e_up[...], preferred_element_type=F32)
        hidden = (jax.nn.silu(g) * u).astype(BF16)
        for n in range(4):
            cols = slice(n * 512, n * 512 + 512)
            produced[rows, cols] = jnp.dot(
                hidden, e_down[:, cols], preferred_element_type=F32
            ).astype(BF16)

    for g in range(GROUPS):
        wait_group(received, recv_sem.at[g], g * GROUP_ROWS, GROUP_ROWS)
        run_group(g * GROUP_ROWS)
        for i in range(g * GROUP_DEV, (g + 1) * GROUP_DEV):
            if i == 0:
                pltpu.make_async_copy(
                    produced.at[slot(0), :], returned.at[slot(0), :], back_recv_sem.at[0]
                ).start()
            else:
                back(i)

    def add_group(first):
        rows = pl.ds(first, GROUP_ROWS)
        left = jnp.concatenate([weight_hi[rows, :], weight_lo[rows, :]], axis=1)
        for n in range(4):
            cols = slice(n * 512, n * 512 + 512)
            both = lax.dot_general(
                left, returned[rows, cols], TN, preferred_element_type=F32
            )
            total[:, cols] += both[:64] + both[64:]

    wait_group(returned, back_recv_sem.at[0], 0, GROUP_ROWS)
    add_group(0)

    def add_one(g, carry):
        first = pl.multiple_of(g * GROUP_ROWS, GROUP_ROWS)
        wait_group(returned, back_recv_sem.at[g], first, GROUP_ROWS)
        add_group(first)
        return carry

    lax.fori_loop(1, GROUPS, add_one, 0)

    combined = total[...]
    out_ref[...] = (
        resid_mid[...].astype(F32)
        + combined * inv_rms(combined) * out_gain_ref[...]
    ).astype(BF16)
    wait_group(s_gate, send_sem, 0, (SLOTS - CAP) * 4)
    wait_group(s_gate, back_send_sem, 0, (SLOTS - CAP) * 4)


def layer(small, wide):
    vmem = pl.BlockSpec(memory_space=pltpu.VMEM)
    hbm = pl.BlockSpec(memory_space=pl.ANY)
    state = pltpu.VMEM((64, 4096), F32)
    row_major = pltpu.VMEM((2048, 512), BF16)
    down = pltpu.VMEM((512, 2048), BF16)
    mixer = pltpu.VMEM((1024, 2048), BF16)
    slots = pltpu.VMEM((SLOTS, 2048), BF16)
    table = pltpu.VMEM((SLOTS, 64), BF16)
    dma = pltpu.SemaphoreType.DMA
    return pl.pallas_call(
        layer_kernel,
        out_shape=(
            jax.ShapeDtypeStruct((64, 2048), BF16),
            jax.ShapeDtypeStruct((64, 4096), F32),
            jax.ShapeDtypeStruct((64, 4096), F32),
        ),
        in_specs=[hbm] * (len(small) + len(wide)),
        out_specs=(vmem, vmem, vmem),
        scratch_shapes=[pltpu.VMEM(shape, kind) for _, shape, kind in SMALL]
        + [
            state,
            state,
            pltpu.VMEM((64, 1024), BF16),
            mixer,
            mixer,
            row_major,
            row_major,
            down,
            row_major,
            row_major,
            down,
            pltpu.VMEM((64, 2048), F32),
            pltpu.VMEM((64, 2048), BF16),
            pltpu.VMEM((64, 2048), BF16),
            table,
            table,
            table,
            pltpu.VMEM((64, 2048), F32),
            slots,
            slots,
            slots,
            slots,
            dma((len(SMALL) + 2 * STATE_PARTS + 14,)),
            dma,
            dma((GROUPS,)),
            dma,
            dma((GROUPS,)),
            pltpu.SemaphoreType.REGULAR,
            pltpu.SemaphoreType.REGULAR,
        ],
        compiler_params=pltpu.CompilerParams(
            collective_id=0, has_side_effects=True, vmem_limit_bytes=42 * 2**20
        ),
        name="layer",
    )(*map(keep, small), *map(keep, wide))


def store_kernel(out_vmem, re_vmem, im_vmem, out_ref, re_ref, im_ref, sem):
    copies = [
        pltpu.make_async_copy(src, dst, sem.at[i])
        for i, (src, dst) in enumerate(
            ((re_vmem, re_ref), (im_vmem, im_ref), (out_vmem, out_ref))
        )
    ]
    for copy in copies:
        copy.start()
    for copy in copies:
        copy.wait()


def store(*arrays):
    return pl.pallas_call(
        store_kernel,
        out_shape=tuple(jax.ShapeDtypeStruct(a.shape, a.dtype) for a in arrays),
        in_specs=[pl.BlockSpec(memory_space=pltpu.VMEM)] * 3,
        out_specs=(pl.BlockSpec(memory_space=pl.ANY),) * 3,
        scratch_shapes=[pltpu.SemaphoreType.DMA((3,))],
        compiler_params=pltpu.CompilerParams(vmem_limit_bytes=2**20),
        name="store",
    )(*arrays)


def per_device(
    residual,
    branch_in,
    state_real,
    state_imag,
    decay_rate,
    frequency,
    log_step,
    input_real,
    input_imag,
    output_matrix_real,
    output_matrix_imaginary,
    skip_gain,
    glu_value,
    glu_gate,
    mix_gain,
    moe_in_gain,
    moe_out_gain,
    routes,
    route_weights,
    expert_gate,
    expert_up,
    expert_down,
    shared_gate,
    shared_up,
    shared_down,
):
    small = (
        log_step.reshape(1, 64),
        decay_rate,
        frequency,
        jnp.transpose(routes),
        jnp.transpose(route_weights),
        branch_in,
        jnp.transpose(input_real, (0, 2, 1)).reshape(1024, 64),
        jnp.transpose(input_imag, (0, 2, 1)).reshape(1024, 64),
        output_matrix_real.reshape(1024, 64),
        output_matrix_imaginary.reshape(1024, 64),
        skip_gain.reshape(1, 1024),
        residual,
        mix_gain.reshape(1, 2048),
        moe_in_gain.reshape(1, 2048),
        moe_out_gain.reshape(1, 2048),
    )
    wide = (
        state_real,
        state_imag,
        glu_value,
        glu_gate,
        expert_gate.reshape(2048, 512),
        expert_up.reshape(2048, 512),
        expert_down.reshape(512, 2048),
        shared_gate,
        shared_up,
        shared_down,
    )
    return store(*layer(small, wide))


def solution(mesh):
    return jax.shard_map(
        per_device,
        mesh=mesh,
        in_specs=(
            P("ep", None),
            P("ep", None),
            P("ep", None),
            P("ep", None),
            P(),
            P(),
            P(),
            P(),
            P(),
            P(),
            P(),
            P(),
            P(),
            P(),
            P(),
            P(),
            P(),
            P("ep", None),
            P("ep", None),
            P("ep", None, None),
            P("ep", None, None),
            P("ep", None, None),
            P(),
            P(),
            P(),
        ),
        out_specs=(P("ep", None), P("ep", None), P("ep", None)),
        check_vma=False,
    )
```

```python
import functools

import jax
import jax.numpy as jnp
from jax import lax
from jax.experimental import pallas as pl
from jax.experimental.pallas import tpu as pltpu
from jax.sharding import PartitionSpec as P

MESH = pl.DeviceIdType.MESH
F32 = jnp.float32
BF16 = jnp.bfloat16
EPS = 1e-06
N_DEV = 128
CAP = 4
SLOTS = N_DEV * CAP


def send_order():
    def length(o):
        return sum(min(d, 4 - d) for d in (o % 4, o // 4 % 4, o // 16))

    order = [0]
    for far in sorted(range(1, 64), key=lambda o: -length(o)):
        x, y, z = far % 4, far // 4 % 4, far // 16
        for a, b, c in ((x, y, z), (y, z, x), (z, x, y)):
            for sign in (1, -1):
                image = (sign * a) % 4 + (sign * b) % 4 * 4 + (sign * c) % 4 * 16
                if image not in order:
                    order.append(image)
    return tuple(2 * o + core for o in order for core in (0, 1))


ORDER = send_order()
GROUPS = 4
GROUP_DEV = N_DEV // GROUPS
GROUP_ROWS = SLOTS // GROUPS
NT = (((1,), (1,)), ((), ()))
TN = (((0,), (0,)), ((), ()))


def keep(value):
    return pltpu.with_memory_space_constraint(value, memory_space=pltpu.HBM)


def split_hi_lo(value):
    hi = value.astype(BF16)
    lo = (value - hi.astype(F32)).astype(BF16)
    return hi, lo


def twice(v):
    return jnp.concatenate([v, v], axis=1)


def state_constants(decay, freq, log_step):
    group = lax.broadcasted_iota(jnp.int32, (64, 64), 0)
    lane = lax.broadcasted_iota(jnp.int32, (64, 64), 1)
    column = jnp.sum(
        jnp.where(group == lane, jnp.broadcast_to(log_step, (64, 64)), 0.0),
        axis=1,
        keepdims=True,
    )
    step_size = jnp.exp(column)
    magnitude = jnp.exp(-decay * step_size)
    phase = freq * step_size
    abar_re = magnitude * jnp.cos(phase)
    abar_im = magnitude * jnp.sin(phase)
    denominator = decay * decay + freq * freq
    numer_re = abar_re - 1.0
    coef_re = (abar_im * freq - numer_re * decay) / denominator
    coef_im = (-abar_im * decay - numer_re * freq) / denominator
    return tuple(map(twice, (abar_re, abar_im, coef_re, coef_im)))


def forcing_block(b, constants, masks, feed_ref, in_re_ref, in_im_ref, next_re, next_im):
    coef_re, coef_im = constants[2:]
    bb_re, bb_im = [], []
    for r in range(b * 8, b * 8 + 8):
        own = slice(r * 16, r * 16 + 16)
        b_re = twice(in_re_ref[own, :].astype(F32))
        b_im = twice(in_im_ref[own, :].astype(F32))
        c_re, c_im = coef_re[r : r + 1, :], coef_im[r : r + 1, :]
        bb_re.append(c_re * b_re - c_im * b_im)
        bb_im.append(c_re * b_im + c_im * b_re)
    feed_twice = twice(feed_ref[:, b * 128 : b * 128 + 128])
    lanes = slice(b * 512, b * 512 + 512)
    for parts, out_ref in ((bb_re, next_re), (bb_im, next_im)):
        hi, lo = split_hi_lo(jnp.concatenate(parts, axis=0))
        table = jnp.concatenate(
            [
                jnp.concatenate([hi * mask for mask in masks], axis=1),
                jnp.concatenate([lo * mask for mask in masks], axis=1),
            ],
            axis=0,
        )
        out_ref[:, lanes] = jnp.dot(feed_twice, table, preferred_element_type=F32)


def state_block(
    b,
    constants,
    masks,
    feed_ref,
    re_ref,
    im_ref,
    out_re_ref,
    out_im_ref,
    skip_ref,
    next_re,
    next_im,
    act_ref,
):
    abar_re, abar_im = constants[:2]
    low_half = lax.broadcasted_iota(jnp.int32, (1, 128), 1) < 64
    here = slice(b * 128, b * 128 + 128)
    his, los = [[], []], [[], []]
    for q in range(4):
        r0 = b * 8 + 2 * q
        a_re = jnp.where(low_half, abar_re[r0 : r0 + 1, :], abar_re[r0 + 1 : r0 + 2, :])
        a_im = jnp.where(low_half, abar_im[r0 : r0 + 1, :], abar_im[r0 + 1 : r0 + 2, :])
        lanes = slice(b * 512 + q * 128, b * 512 + q * 128 + 128)
        old_re, old_im = re_ref[:, lanes], im_ref[:, lanes]
        new_re = a_re * old_re - a_im * old_im + next_re[:, lanes]
        new_im = a_re * old_im + a_im * old_re + next_im[:, lanes]
        next_re[:, lanes] = new_re
        next_im[:, lanes] = new_im
        for i, new in enumerate((new_re, new_im)):
            hi, lo = split_hi_lo(new)
            his[i].append(hi)
            los[i].append(lo)
    o_re = twice(out_re_ref[here, :].astype(F32)).astype(BF16)
    o_im = twice(-out_im_ref[here, :].astype(F32)).astype(BF16)
    w = jnp.concatenate(
        [o_re * mask for mask in masks] + [o_im * mask for mask in masks], axis=1
    )
    left = jnp.concatenate(
        [
            jnp.concatenate(his[0] + his[1], axis=1),
            jnp.concatenate(los[0] + los[1], axis=1),
        ],
        axis=0,
    )
    both = lax.dot_general(left, w, NT, preferred_element_type=F32)
    mixed = both[:64] + both[64:] + skip_ref[:, here] * feed_ref[:, here].astype(F32)
    act_ref[:, here] = jax.nn.gelu(mixed).astype(BF16)


def torus_add(me, off):
    core = lax.rem(me + off, 2)
    x = lax.rem(me // 2 + off // 2, 4)
    y = lax.rem(me // 8 + off // 8, 4)
    z = lax.rem(me // 32 + off // 32, 4)
    return ((z * 4 + y) * 4 + x) * 2 + core


def torus_sub(me, off):
    core = lax.rem(me + off, 2)
    x = lax.rem(me // 2 + 4 - lax.rem(off // 2, 4), 4)
    y = lax.rem(me // 8 + 4 - lax.rem(off // 8, 4), 4)
    z = lax.rem(me // 32 + 4 - off // 32, 4)
    return ((z * 4 + y) * 4 + x) * 2 + core


def inv_rms(v):
    return lax.rsqrt(jnp.mean(v * v, axis=-1, keepdims=True) + EPS)


SMALL = (
    ("log_step", (1, 64), F32),
    ("decay", (64, 64), F32),
    ("freq", (64, 64), F32),
    ("routes", (6, 64), jnp.int32),
    ("weights", (6, 64), F32),
    ("feed", (64, 1024), BF16),
    ("in_re", (1024, 64), BF16),
    ("in_im", (1024, 64), BF16),
    ("out_re", (1024, 64), BF16),
    ("out_im", (1024, 64), BF16),
    ("skip", (1, 1024), F32),
    ("resid", (64, 2048), BF16),
    ("mix_gain", (1, 2048), F32),
    ("in_gain", (1, 2048), F32),
    ("out_gain", (1, 2048), F32),
)
STATE_PARTS = 4


def layer_kernel(*refs):
    n = len(SMALL)
    small_hbm, refs = refs[:n], refs[n:]
    (
        re_hbm,
        im_hbm,
        glu_value_hbm,
        glu_gate_hbm,
        e_gate_hbm,
        e_up_hbm,
        e_down_hbm,
        s_gate_hbm,
        s_up_hbm,
        s_down_hbm,
        out_ref,
        next_re,
        next_im,
    ) = refs[:13]
    refs = refs[13:]
    small, refs = refs[:n], refs[n:]
    (
        log_step_ref,
        decay_ref,
        freq_ref,
        routes_ref,
        weights_ref,
        feed_ref,
        in_re_ref,
        in_im_ref,
        out_re_ref,
        out_im_ref,
        skip_ref,
        resid_ref,
        mix_gain_ref,
        in_gain_ref,
        out_gain_ref,
    ) = small
    (
        old_re,
        old_im,
        act_ref,
        glu_value,
        glu_gate,
        e_gate,
        e_up,
        e_down,
        s_gate,
        s_up,
        s_down,
        branch,
        resid_mid,
        normed,
        pick,
        weight_hi,
        weight_lo,
        total,
        outgoing,
        received,
        produced,
        returned,
        load_sem,
        send_sem,
        recv_sem,
        back_send_sem,
        back_recv_sem,
        all_sem,
    ) = refs
    me = lax.axis_index("ep")
    barrier = pltpu.get_barrier_semaphore()

    plane = [torus_add(me, o) for o in range(1, 32)]
    line_z = [torus_add(me, 32 * o) for o in range(1, 4)]

    def greet(sem, devices):
        for device in devices:
            pl.semaphore_signal(
                sem, inc=1, device_id=(device,), device_id_type=MESH
            )

    greet(barrier, plane + line_z)

    loads = []

    def load(src, dst):
        copy = pltpu.make_async_copy(src, dst, load_sem.at[len(loads)])
        copy.start()
        loads.append(copy)
        return copy

    small_loads = [load(src, dst) for src, dst in zip(small_hbm, small)]
    state_loads = []
    for part in range(STATE_PARTS):
        cols = pl.ds(part * 4096 // STATE_PARTS, 4096 // STATE_PARTS)
        state_loads.append(
            (
                load(re_hbm.at[:, cols], old_re.at[:, cols]),
                load(im_hbm.at[:, cols], old_im.at[:, cols]),
            )
        )
    value_load = load(glu_value_hbm, glu_value)
    gate_load = load(glu_gate_hbm, glu_gate)
    row_group = lax.broadcasted_iota(jnp.int32, (128, 128), 0) // 16
    lane_half = lax.broadcasted_iota(jnp.int32, (128, 128), 1) // 64
    masks = [
        jnp.where(row_group == 2 * q + lane_half, 1.0, 0.0).astype(BF16)
        for q in range(4)
    ]
    for copy in small_loads[:5]:
        copy.wait()
    constants = state_constants(decay_ref[...], freq_ref[...], log_step_ref[...])

    routes = routes_ref[...]
    rel = (
        jnp.bitwise_and(routes + me, 1)
        + jnp.bitwise_and((routes >> 1) + 4 - lax.rem(me // 2, 4), 3) * 2
        + jnp.bitwise_and((routes >> 3) + 4 - lax.rem(me // 8, 4), 3) * 8
        + jnp.bitwise_and((routes >> 5) + 4 - me // 32, 3) * 32
    )
    position = jnp.zeros_like(rel)
    for i in range(1, N_DEV):
        position = jnp.where(rel == ORDER[i], i, position)
    row = lax.broadcasted_iota(jnp.int32, (SLOTS, 64), 0)
    row_pos = row >> 2
    row_rank = jnp.bitwise_and(row, 3).astype(F32)
    named = jnp.zeros((SLOTS, 64), F32)
    weight = jnp.zeros((SLOTS, 64), F32)
    for k in range(6):
        hit = row_pos == position[k : k + 1, :]
        named = jnp.where(hit, 1.0, named)
        weight = jnp.where(hit, weights_ref[k : k + 1, :], weight)
    earlier = (
        lax.broadcasted_iota(jnp.int32, (64, 64), 0)
        < lax.broadcasted_iota(jnp.int32, (64, 64), 1)
    ).astype(BF16)
    rank = jnp.dot(named.astype(BF16), earlier, preferred_element_type=F32)
    chosen = rank == row_rank
    pick[...] = jnp.where(chosen, named, 0.0).astype(BF16)
    hi, lo = split_hi_lo(jnp.where(chosen, weight, 0.0))
    weight_hi[...] = hi
    weight_lo[...] = lo

    for copy in small_loads[5:]:
        copy.wait()
    for b in range(8):
        forcing_block(
            b, constants, masks, feed_ref, in_re_ref, in_im_ref, next_re, next_im
        )
    for part in range(STATE_PARTS):
        for copy in state_loads[part]:
            copy.wait()
        for b in range(part * 8 // STATE_PARTS, (part + 1) * 8 // STATE_PARTS):
            state_block(
                b,
                constants,
                masks,
                feed_ref,
                old_re,
                old_im,
                out_re_ref,
                out_im_ref,
                skip_ref,
                next_re,
                next_im,
                act_ref,
            )
        if part == 1:
            pl.semaphore_wait(barrier, 34)
            greet(all_sem, line_z)
    s_loads = [load(s_gate_hbm, s_gate), load(s_up_hbm, s_up), load(s_down_hbm, s_down)]
    e_loads = [load(e_gate_hbm, e_gate), load(e_up_hbm, e_up), load(e_down_hbm, e_down)]

    act = act_ref[...]
    square = jnp.zeros((64, 1), F32)
    value_load.wait()
    for n in range(4):
        cols = slice(n * 512, n * 512 + 512)
        branch[:, cols] = jnp.dot(act, glu_value[:, cols], preferred_element_type=F32)
    gate_load.wait()
    for n in range(4):
        cols = slice(n * 512, n * 512 + 512)
        gate_part = jnp.dot(act, glu_gate[:, cols], preferred_element_type=F32)
        part = branch[:, cols] * jax.nn.sigmoid(gate_part)
        branch[:, cols] = part
        square = square + jnp.sum(part * part, axis=-1, keepdims=True)
    scale = lax.rsqrt(square * (1.0 / 2048) + EPS)
    mid = (
        resid_ref[...].astype(F32) + branch[...] * scale * mix_gain_ref[...]
    ).astype(BF16)
    resid_mid[...] = mid
    mid = mid.astype(F32)
    normed[...] = (mid * inv_rms(mid) * in_gain_ref[...]).astype(BF16)

    def slot(i):
        return pl.ds(i * CAP, CAP)

    for g in range(GROUPS):
        rows = slice(g * GROUP_ROWS, (g + 1) * GROUP_ROWS)
        outgoing[rows, :] = jnp.dot(
            pick[rows, :], normed[...], preferred_element_type=F32
        ).astype(BF16)
        if g == 0:
            pl.semaphore_wait(all_sem, 3)
            pltpu.make_async_copy(
                outgoing.at[slot(0), :], received.at[slot(0), :], recv_sem.at[0]
            ).start()
        for i in range(max(1, g * GROUP_DEV), (g + 1) * GROUP_DEV):
            pltpu.make_async_remote_copy(
                src_ref=outgoing.at[slot(i), :],
                dst_ref=received.at[slot(i), :],
                send_sem=send_sem,
                recv_sem=recv_sem.at[g],
                device_id=(torus_add(me, ORDER[i]),),
                device_id_type=MESH,
            ).start()

    for copy in s_loads:
        copy.wait()
    x = normed[...]
    g = jnp.dot(x, s_gate[...], preferred_element_type=F32)
    u = jnp.dot(x, s_up[...], preferred_element_type=F32)
    hidden = (jax.nn.silu(g) * u).astype(BF16)
    for n in range(4):
        cols = slice(n * 512, n * 512 + 512)
        total[:, cols] = jnp.dot(hidden, s_down[:, cols], preferred_element_type=F32)
    for copy in e_loads:
        copy.wait()

    def wait_group(buffer, sem, first, rows):
        part = buffer.at[pl.ds(first, rows), :]
        pltpu.make_async_copy(part, part, sem).wait()

    def back(i):
        pltpu.make_async_remote_copy(
            src_ref=produced.at[slot(i), :],
            dst_ref=returned.at[slot(i), :],
            send_sem=back_send_sem,
            recv_sem=back_recv_sem.at[i // GROUP_DEV],
            device_id=(torus_sub(me, ORDER[i]),),
            device_id_type=MESH,
        ).start()

    def run_group(first):
        rows = pl.ds(first, GROUP_ROWS)
        x = received[rows, :]
        g = jnp.dot(x, e_gate[...], preferred_element_type=F32)
        u = jnp.dot(x, e_up[...], preferred_element_type=F32)
        hidden = (jax.nn.silu(g) * u).astype(BF16)
        for n in range(4):
            cols = slice(n * 512, n * 512 + 512)
            produced[rows, cols] = jnp.dot(
                hidden, e_down[:, cols], preferred_element_type=F32
            ).astype(BF16)

    for g in range(GROUPS):
        wait_group(received, recv_sem.at[g], g * GROUP_ROWS, GROUP_ROWS)
        run_group(g * GROUP_ROWS)
        for i in range(g * GROUP_DEV, (g + 1) * GROUP_DEV):
            if i == 0:
                pltpu.make_async_copy(
                    produced.at[slot(0), :], returned.at[slot(0), :], back_recv_sem.at[0]
                ).start()
            else:
                back(i)

    def add_group(first):
        rows = pl.ds(first, GROUP_ROWS)
        left = jnp.concatenate([weight_hi[rows, :], weight_lo[rows, :]], axis=1)
        for n in range(4):
            cols = slice(n * 512, n * 512 + 512)
            both = lax.dot_general(
                left, returned[rows, cols], TN, preferred_element_type=F32
            )
            total[:, cols] += both[:64] + both[64:]

    wait_group(returned, back_recv_sem.at[0], 0, GROUP_ROWS)
    add_group(0)

    def add_one(g, carry):
        first = pl.multiple_of(g * GROUP_ROWS, GROUP_ROWS)
        wait_group(returned, back_recv_sem.at[g], first, GROUP_ROWS)
        add_group(first)
        return carry

    lax.fori_loop(1, GROUPS, add_one, 0)

    combined = total[...]
    out_ref[...] = (
        resid_mid[...].astype(F32)
        + combined * inv_rms(combined) * out_gain_ref[...]
    ).astype(BF16)
    wait_group(s_gate, send_sem, 0, (SLOTS - CAP) * 4)
    wait_group(s_gate, back_send_sem, 0, (SLOTS - CAP) * 4)


def layer(small, wide):
    vmem = pl.BlockSpec(memory_space=pltpu.VMEM)
    hbm = pl.BlockSpec(memory_space=pl.ANY)
    state = pltpu.VMEM((64, 4096), F32)
    row_major = pltpu.VMEM((2048, 512), BF16)
    down = pltpu.VMEM((512, 2048), BF16)
    mixer = pltpu.VMEM((1024, 2048), BF16)
    slots = pltpu.VMEM((SLOTS, 2048), BF16)
    table = pltpu.VMEM((SLOTS, 64), BF16)
    dma = pltpu.SemaphoreType.DMA
    return pl.pallas_call(
        layer_kernel,
        out_shape=(
            jax.ShapeDtypeStruct((64, 2048), BF16),
            jax.ShapeDtypeStruct((64, 4096), F32),
            jax.ShapeDtypeStruct((64, 4096), F32),
        ),
        in_specs=[hbm] * (len(small) + len(wide)),
        out_specs=(vmem, vmem, vmem),
        scratch_shapes=[pltpu.VMEM(shape, kind) for _, shape, kind in SMALL]
        + [
            state,
            state,
            pltpu.VMEM((64, 1024), BF16),
            mixer,
            mixer,
            row_major,
            row_major,
            down,
            row_major,
            row_major,
            down,
            pltpu.VMEM((64, 2048), F32),
            pltpu.VMEM((64, 2048), BF16),
            pltpu.VMEM((64, 2048), BF16),
            table,
            table,
            table,
            pltpu.VMEM((64, 2048), F32),
            slots,
            slots,
            slots,
            slots,
            dma((len(SMALL) + 2 * STATE_PARTS + 14,)),
            dma,
            dma((GROUPS,)),
            dma,
            dma((GROUPS,)),
            pltpu.SemaphoreType.REGULAR,
        ],
        compiler_params=pltpu.CompilerParams(
            collective_id=0, has_side_effects=True, vmem_limit_bytes=42 * 2**20
        ),
        name="layer",
    )(*map(keep, small), *map(keep, wide))


def store_kernel(out_vmem, re_vmem, im_vmem, out_ref, re_ref, im_ref, sem):
    copies = [
        pltpu.make_async_copy(src, dst, sem.at[i])
        for i, (src, dst) in enumerate(
            ((re_vmem, re_ref), (im_vmem, im_ref), (out_vmem, out_ref))
        )
    ]
    for copy in copies:
        copy.start()
    for copy in copies:
        copy.wait()


def store(*arrays):
    return pl.pallas_call(
        store_kernel,
        out_shape=tuple(jax.ShapeDtypeStruct(a.shape, a.dtype) for a in arrays),
        in_specs=[pl.BlockSpec(memory_space=pltpu.VMEM)] * 3,
        out_specs=(pl.BlockSpec(memory_space=pl.ANY),) * 3,
        scratch_shapes=[pltpu.SemaphoreType.DMA((3,))],
        compiler_params=pltpu.CompilerParams(vmem_limit_bytes=2**20),
        name="store",
    )(*arrays)


def per_device(
    residual,
    branch_in,
    state_real,
    state_imag,
    decay_rate,
    frequency,
    log_step,
    input_real,
    input_imag,
    output_matrix_real,
    output_matrix_imaginary,
    skip_gain,
    glu_value,
    glu_gate,
    mix_gain,
    moe_in_gain,
    moe_out_gain,
    routes,
    route_weights,
    expert_gate,
    expert_up,
    expert_down,
    shared_gate,
    shared_up,
    shared_down,
):
    small = (
        log_step.reshape(1, 64),
        decay_rate,
        frequency,
        jnp.transpose(routes),
        jnp.transpose(route_weights),
        branch_in,
        jnp.transpose(input_real, (0, 2, 1)).reshape(1024, 64),
        jnp.transpose(input_imag, (0, 2, 1)).reshape(1024, 64),
        output_matrix_real.reshape(1024, 64),
        output_matrix_imaginary.reshape(1024, 64),
        skip_gain.reshape(1, 1024),
        residual,
        mix_gain.reshape(1, 2048),
        moe_in_gain.reshape(1, 2048),
        moe_out_gain.reshape(1, 2048),
    )
    wide = (
        state_real,
        state_imag,
        glu_value,
        glu_gate,
        expert_gate.reshape(2048, 512),
        expert_up.reshape(2048, 512),
        expert_down.reshape(512, 2048),
        shared_gate,
        shared_up,
        shared_down,
    )
    return store(*layer(small, wide))


def solution(mesh):
    return jax.shard_map(
        per_device,
        mesh=mesh,
        in_specs=(
            P("ep", None),
            P("ep", None),
            P("ep", None),
            P("ep", None),
            P(),
            P(),
            P(),
            P(),
            P(),
            P(),
            P(),
            P(),
            P(),
            P(),
            P(),
            P(),
            P(),
            P("ep", None),
            P("ep", None),
            P("ep", None, None),
            P("ep", None, None),
            P("ep", None, None),
            P(),
            P(),
            P(),
        ),
        out_specs=(P("ep", None), P("ep", None), P("ep", None)),
        check_vma=False,
    )
```

```python
import functools

import jax
import jax.numpy as jnp
from jax import lax
from jax.experimental import pallas as pl
from jax.experimental.pallas import tpu as pltpu
from jax.sharding import PartitionSpec as P

MESH = pl.DeviceIdType.MESH
F32 = jnp.float32
BF16 = jnp.bfloat16
EPS = 1e-06
N_DEV = 128
CAP = 4
SLOTS = N_DEV * CAP


def send_order():
    def length(o):
        return sum(min(d, 4 - d) for d in (o % 4, o // 4 % 4, o // 16))

    order = [0]
    for far in sorted(range(1, 64), key=lambda o: -length(o)):
        x, y, z = far % 4, far // 4 % 4, far // 16
        for a, b, c in ((x, y, z), (y, z, x), (z, x, y)):
            for sign in (1, -1):
                image = (sign * a) % 4 + (sign * b) % 4 * 4 + (sign * c) % 4 * 16
                if image not in order:
                    order.append(image)
    return tuple(2 * o + core for o in order for core in (0, 1))


ORDER = send_order()
GROUPS = 4
GROUP_DEV = N_DEV // GROUPS
GROUP_ROWS = SLOTS // GROUPS
NT = (((1,), (1,)), ((), ()))
TN = (((0,), (0,)), ((), ()))


def keep(value):
    return pltpu.with_memory_space_constraint(value, memory_space=pltpu.HBM)


def split_hi_lo(value):
    hi = value.astype(BF16)
    lo = (value - hi.astype(F32)).astype(BF16)
    return hi, lo


def twice(v):
    return jnp.concatenate([v, v], axis=1)


def state_constants(decay, freq, log_step):
    group = lax.broadcasted_iota(jnp.int32, (64, 64), 0)
    lane = lax.broadcasted_iota(jnp.int32, (64, 64), 1)
    column = jnp.sum(
        jnp.where(group == lane, jnp.broadcast_to(log_step, (64, 64)), 0.0),
        axis=1,
        keepdims=True,
    )
    step_size = jnp.exp(column)
    magnitude = jnp.exp(-decay * step_size)
    phase = freq * step_size
    abar_re = magnitude * jnp.cos(phase)
    abar_im = magnitude * jnp.sin(phase)
    denominator = decay * decay + freq * freq
    numer_re = abar_re - 1.0
    coef_re = (abar_im * freq - numer_re * decay) / denominator
    coef_im = (-abar_im * decay - numer_re * freq) / denominator
    return tuple(map(twice, (abar_re, abar_im, coef_re, coef_im)))


def forcing_block(b, constants, masks, feed_ref, in_re_ref, in_im_ref, next_re, next_im):
    coef_re, coef_im = constants[2:]
    bb_re, bb_im = [], []
    for r in range(b * 8, b * 8 + 8):
        own = slice(r * 16, r * 16 + 16)
        b_re = twice(in_re_ref[own, :].astype(F32))
        b_im = twice(in_im_ref[own, :].astype(F32))
        c_re, c_im = coef_re[r : r + 1, :], coef_im[r : r + 1, :]
        bb_re.append(c_re * b_re - c_im * b_im)
        bb_im.append(c_re * b_im + c_im * b_re)
    feed_twice = twice(feed_ref[:, b * 128 : b * 128 + 128])
    lanes = slice(b * 512, b * 512 + 512)
    for parts, out_ref in ((bb_re, next_re), (bb_im, next_im)):
        hi, lo = split_hi_lo(jnp.concatenate(parts, axis=0))
        table = jnp.concatenate(
            [
                jnp.concatenate([hi * mask for mask in masks], axis=1),
                jnp.concatenate([lo * mask for mask in masks], axis=1),
            ],
            axis=0,
        )
        out_ref[:, lanes] = jnp.dot(feed_twice, table, preferred_element_type=F32)


def state_block(
    b,
    constants,
    masks,
    feed_ref,
    re_ref,
    im_ref,
    out_re_ref,
    out_im_ref,
    skip_ref,
    next_re,
    next_im,
    act_ref,
):
    abar_re, abar_im = constants[:2]
    low_half = lax.broadcasted_iota(jnp.int32, (1, 128), 1) < 64
    here = slice(b * 128, b * 128 + 128)
    his, los = [[], []], [[], []]
    for q in range(4):
        r0 = b * 8 + 2 * q
        a_re = jnp.where(low_half, abar_re[r0 : r0 + 1, :], abar_re[r0 + 1 : r0 + 2, :])
        a_im = jnp.where(low_half, abar_im[r0 : r0 + 1, :], abar_im[r0 + 1 : r0 + 2, :])
        lanes = slice(b * 512 + q * 128, b * 512 + q * 128 + 128)
        old_re, old_im = re_ref[:, lanes], im_ref[:, lanes]
        new_re = a_re * old_re - a_im * old_im + next_re[:, lanes]
        new_im = a_re * old_im + a_im * old_re + next_im[:, lanes]
        next_re[:, lanes] = new_re
        next_im[:, lanes] = new_im
        for i, new in enumerate((new_re, new_im)):
            hi, lo = split_hi_lo(new)
            his[i].append(hi)
            los[i].append(lo)
    o_re = twice(out_re_ref[here, :].astype(F32)).astype(BF16)
    o_im = twice(-out_im_ref[here, :].astype(F32)).astype(BF16)
    w = jnp.concatenate(
        [o_re * mask for mask in masks] + [o_im * mask for mask in masks], axis=1
    )
    left = jnp.concatenate(
        [
            jnp.concatenate(his[0] + his[1], axis=1),
            jnp.concatenate(los[0] + los[1], axis=1),
        ],
        axis=0,
    )
    both = lax.dot_general(left, w, NT, preferred_element_type=F32)
    mixed = both[:64] + both[64:] + skip_ref[:, here] * feed_ref[:, here].astype(F32)
    act_ref[:, here] = jax.nn.gelu(mixed).astype(BF16)


def torus_add(me, off):
    core = lax.rem(me + off, 2)
    x = lax.rem(me // 2 + off // 2, 4)
    y = lax.rem(me // 8 + off // 8, 4)
    z = lax.rem(me // 32 + off // 32, 4)
    return ((z * 4 + y) * 4 + x) * 2 + core


def torus_sub(me, off):
    core = lax.rem(me + off, 2)
    x = lax.rem(me // 2 + 4 - lax.rem(off // 2, 4), 4)
    y = lax.rem(me // 8 + 4 - lax.rem(off // 8, 4), 4)
    z = lax.rem(me // 32 + 4 - off // 32, 4)
    return ((z * 4 + y) * 4 + x) * 2 + core


def inv_rms(v):
    return lax.rsqrt(jnp.mean(v * v, axis=-1, keepdims=True) + EPS)


SMALL = (
    ("log_step", (1, 64), F32),
    ("decay", (64, 64), F32),
    ("freq", (64, 64), F32),
    ("routes", (6, 64), jnp.int32),
    ("weights", (6, 64), F32),
    ("feed", (64, 1024), BF16),
    ("in_re", (1024, 64), BF16),
    ("in_im", (1024, 64), BF16),
    ("out_re", (1024, 64), BF16),
    ("out_im", (1024, 64), BF16),
    ("skip", (1, 1024), F32),
    ("resid", (64, 2048), BF16),
    ("mix_gain", (1, 2048), F32),
    ("in_gain", (1, 2048), F32),
    ("out_gain", (1, 2048), F32),
)
STATE_PARTS = 2


def layer_kernel(*refs):
    n = len(SMALL)
    small_hbm, refs = refs[:n], refs[n:]
    (
        re_hbm,
        im_hbm,
        glu_value_hbm,
        glu_gate_hbm,
        e_gate_hbm,
        e_up_hbm,
        e_down_hbm,
        s_gate_hbm,
        s_up_hbm,
        s_down_hbm,
        out_ref,
        next_re,
        next_im,
    ) = refs[:13]
    refs = refs[13:]
    small, refs = refs[:n], refs[n:]
    (
        log_step_ref,
        decay_ref,
        freq_ref,
        routes_ref,
        weights_ref,
        feed_ref,
        in_re_ref,
        in_im_ref,
        out_re_ref,
        out_im_ref,
        skip_ref,
        resid_ref,
        mix_gain_ref,
        in_gain_ref,
        out_gain_ref,
    ) = small
    (
        old_re,
        old_im,
        act_ref,
        glu_value,
        glu_gate,
        e_gate,
        e_up,
        e_down,
        s_gate,
        s_up,
        s_down,
        branch,
        resid_mid,
        normed,
        slot_position,
        pick,
        weight_hi,
        weight_lo,
        total,
        outgoing,
        received,
        produced,
        returned,
        load_sem,
        send_sem,
        recv_sem,
        back_send_sem,
        back_recv_sem,
        all_sem,
    ) = refs
    me = lax.axis_index("ep")
    barrier = pltpu.get_barrier_semaphore()

    plane = [torus_add(me, o) for o in range(1, 32)]
    line_z = [torus_add(me, 32 * o) for o in range(1, 4)]

    def greet(sem, devices):
        for device in devices:
            pl.semaphore_signal(
                sem, inc=1, device_id=(device,), device_id_type=MESH
            )

    greet(barrier, plane + line_z)

    loads = []

    def load(src, dst):
        copy = pltpu.make_async_copy(src, dst, load_sem.at[len(loads)])
        copy.start()
        loads.append(copy)
        return copy

    small_loads = [load(src, dst) for src, dst in zip(small_hbm, small)]
    state_loads = []
    for part in range(STATE_PARTS):
        cols = pl.ds(part * 4096 // STATE_PARTS, 4096 // STATE_PARTS)
        state_loads.append(
            (
                load(re_hbm.at[:, cols], old_re.at[:, cols]),
                load(im_hbm.at[:, cols], old_im.at[:, cols]),
            )
        )
    value_load = load(glu_value_hbm, glu_value)
    gate_load = load(glu_gate_hbm, glu_gate)
    row_group = lax.broadcasted_iota(jnp.int32, (128, 128), 0) // 16
    lane_half = lax.broadcasted_iota(jnp.int32, (128, 128), 1) // 64
    masks = [
        jnp.where(row_group == 2 * q + lane_half, 1.0, 0.0).astype(BF16)
        for q in range(4)
    ]
    for copy in small_loads[:5]:
        copy.wait()
    constants = state_constants(decay_ref[...], freq_ref[...], log_step_ref[...])

    routes = routes_ref[...]
    rel = (
        jnp.bitwise_and(routes + me, 1)
        + jnp.bitwise_and((routes >> 1) + 4 - lax.rem(me // 2, 4), 3) * 2
        + jnp.bitwise_and((routes >> 3) + 4 - lax.rem(me // 8, 4), 3) * 8
        + jnp.bitwise_and((routes >> 5) + 4 - me // 32, 3) * 32
    )
    position = jnp.zeros_like(rel)
    for i in range(1, N_DEV):
        position = jnp.where(rel == ORDER[i], i, position)
    row = lax.broadcasted_iota(jnp.int32, (SLOTS, 64), 0)
    row_pos = row >> 2
    row_rank = jnp.bitwise_and(row, 3).astype(F32)
    named = jnp.zeros((SLOTS, 64), F32)
    for k in range(6):
        named = jnp.where(row_pos == position[k : k + 1, :], 1.0, named)
    earlier = (
        lax.broadcasted_iota(jnp.int32, (64, 64), 0)
        < lax.broadcasted_iota(jnp.int32, (64, 64), 1)
    ).astype(BF16)
    rank = jnp.dot(named.astype(BF16), earlier, preferred_element_type=F32)
    chosen = rank == row_rank
    pick[...] = jnp.where(chosen, named, 0.0).astype(BF16)
    slot_position[...] = position

    for copy in small_loads[5:]:
        copy.wait()
    for b in range(8):
        forcing_block(
            b, constants, masks, feed_ref, in_re_ref, in_im_ref, next_re, next_im
        )
    for part in range(STATE_PARTS):
        for copy in state_loads[part]:
            copy.wait()
        for b in range(part * 8 // STATE_PARTS, (part + 1) * 8 // STATE_PARTS):
            state_block(
                b,
                constants,
                masks,
                feed_ref,
                old_re,
                old_im,
                out_re_ref,
                out_im_ref,
                skip_ref,
                next_re,
                next_im,
                act_ref,
            )
        if part == 0:
            pl.semaphore_wait(barrier, 34)
            greet(all_sem, line_z)
    s_loads = [load(s_gate_hbm, s_gate), load(s_up_hbm, s_up), load(s_down_hbm, s_down)]
    e_loads = [load(e_gate_hbm, e_gate), load(e_up_hbm, e_up), load(e_down_hbm, e_down)]

    act = act_ref[...]
    square = jnp.zeros((64, 1), F32)
    value_load.wait()
    for n in range(4):
        cols = slice(n * 512, n * 512 + 512)
        branch[:, cols] = jnp.dot(act, glu_value[:, cols], preferred_element_type=F32)
    gate_load.wait()
    for n in range(4):
        cols = slice(n * 512, n * 512 + 512)
        gate_part = jnp.dot(act, glu_gate[:, cols], preferred_element_type=F32)
        part = branch[:, cols] * jax.nn.sigmoid(gate_part)
        branch[:, cols] = part
        square = square + jnp.sum(part * part, axis=-1, keepdims=True)
    scale = lax.rsqrt(square * (1.0 / 2048) + EPS)
    mid = (
        resid_ref[...].astype(F32) + branch[...] * scale * mix_gain_ref[...]
    ).astype(BF16)
    resid_mid[...] = mid
    mid = mid.astype(F32)
    normed[...] = (mid * inv_rms(mid) * in_gain_ref[...]).astype(BF16)

    def slot(i):
        return pl.ds(i * CAP, CAP)

    for g in range(GROUPS):
        rows = slice(g * GROUP_ROWS, (g + 1) * GROUP_ROWS)
        outgoing[rows, :] = jnp.dot(
            pick[rows, :], normed[...], preferred_element_type=F32
        ).astype(BF16)
        if g == 0:
            pl.semaphore_wait(all_sem, 3)
            pltpu.make_async_copy(
                outgoing.at[slot(0), :], received.at[slot(0), :], recv_sem.at[0]
            ).start()
        for i in range(max(1, g * GROUP_DEV), (g + 1) * GROUP_DEV):
            pltpu.make_async_remote_copy(
                src_ref=outgoing.at[slot(i), :],
                dst_ref=received.at[slot(i), :],
                send_sem=send_sem,
                recv_sem=recv_sem.at[g],
                device_id=(torus_add(me, ORDER[i]),),
                device_id_type=MESH,
            ).start()

    weight = jnp.zeros((SLOTS, 64), F32)
    for k in range(6):
        hit = row_pos == slot_position[k : k + 1, :]
        weight = jnp.where(hit, weights_ref[k : k + 1, :], weight)
    hi, lo = split_hi_lo(weight * pick[...].astype(F32))
    weight_hi[...] = hi
    weight_lo[...] = lo
    for copy in s_loads:
        copy.wait()
    x = normed[...]
    g = jnp.dot(x, s_gate[...], preferred_element_type=F32)
    u = jnp.dot(x, s_up[...], preferred_element_type=F32)
    hidden = (jax.nn.silu(g) * u).astype(BF16)
    for n in range(4):
        cols = slice(n * 512, n * 512 + 512)
        total[:, cols] = jnp.dot(hidden, s_down[:, cols], preferred_element_type=F32)
    for copy in e_loads:
        copy.wait()

    def wait_group(buffer, sem, first, rows):
        part = buffer.at[pl.ds(first, rows), :]
        pltpu.make_async_copy(part, part, sem).wait()

    def back(i):
        pltpu.make_async_remote_copy(
            src_ref=produced.at[slot(i), :],
            dst_ref=returned.at[slot(i), :],
            send_sem=back_send_sem,
            recv_sem=back_recv_sem.at[i // GROUP_DEV],
            device_id=(torus_sub(me, ORDER[i]),),
            device_id_type=MESH,
        ).start()

    def run_group(first):
        rows = pl.ds(first, GROUP_ROWS)
        x = received[rows, :]
        g = jnp.dot(x, e_gate[...], preferred_element_type=F32)
        u = jnp.dot(x, e_up[...], preferred_element_type=F32)
        hidden = (jax.nn.silu(g) * u).astype(BF16)
        for n in range(4):
            cols = slice(n * 512, n * 512 + 512)
            produced[rows, cols] = jnp.dot(
                hidden, e_down[:, cols], preferred_element_type=F32
            ).astype(BF16)

    for g in range(GROUPS):
        wait_group(received, recv_sem.at[g], g * GROUP_ROWS, GROUP_ROWS)
        run_group(g * GROUP_ROWS)
        for i in range(g * GROUP_DEV, (g + 1) * GROUP_DEV):
            if i == 0:
                pltpu.make_async_copy(
                    produced.at[slot(0), :], returned.at[slot(0), :], back_recv_sem.at[0]
                ).start()
            else:
                back(i)

    def add_group(first):
        rows = pl.ds(first, GROUP_ROWS)
        left = jnp.concatenate([weight_hi[rows, :], weight_lo[rows, :]], axis=1)
        for n in range(4):
            cols = slice(n * 512, n * 512 + 512)
            both = lax.dot_general(
                left, returned[rows, cols], TN, preferred_element_type=F32
            )
            total[:, cols] += both[:64] + both[64:]

    wait_group(returned, back_recv_sem.at[0], 0, GROUP_ROWS)
    add_group(0)

    def add_one(g, carry):
        first = pl.multiple_of(g * GROUP_ROWS, GROUP_ROWS)
        wait_group(returned, back_recv_sem.at[g], first, GROUP_ROWS)
        add_group(first)
        return carry

    lax.fori_loop(1, GROUPS, add_one, 0)

    combined = total[...]
    out_ref[...] = (
        resid_mid[...].astype(F32)
        + combined * inv_rms(combined) * out_gain_ref[...]
    ).astype(BF16)
    wait_group(s_gate, send_sem, 0, (SLOTS - CAP) * 4)
    wait_group(s_gate, back_send_sem, 0, (SLOTS - CAP) * 4)


def layer(small, wide):
    vmem = pl.BlockSpec(memory_space=pltpu.VMEM)
    hbm = pl.BlockSpec(memory_space=pl.ANY)
    state = pltpu.VMEM((64, 4096), F32)
    row_major = pltpu.VMEM((2048, 512), BF16)
    down = pltpu.VMEM((512, 2048), BF16)
    mixer = pltpu.VMEM((1024, 2048), BF16)
    slots = pltpu.VMEM((SLOTS, 2048), BF16)
    table = pltpu.VMEM((SLOTS, 64), BF16)
    dma = pltpu.SemaphoreType.DMA
    return pl.pallas_call(
        layer_kernel,
        out_shape=(
            jax.ShapeDtypeStruct((64, 2048), BF16),
            jax.ShapeDtypeStruct((64, 4096), F32),
            jax.ShapeDtypeStruct((64, 4096), F32),
        ),
        in_specs=[hbm] * (len(small) + len(wide)),
        out_specs=(vmem, vmem, vmem),
        scratch_shapes=[pltpu.VMEM(shape, kind) for _, shape, kind in SMALL]
        + [
            state,
            state,
            pltpu.VMEM((64, 1024), BF16),
            mixer,
            mixer,
            row_major,
            row_major,
            down,
            row_major,
            row_major,
            down,
            pltpu.VMEM((64, 2048), F32),
            pltpu.VMEM((64, 2048), BF16),
            pltpu.VMEM((64, 2048), BF16),
            pltpu.VMEM((6, 64), jnp.int32),
            table,
            table,
            table,
            pltpu.VMEM((64, 2048), F32),
            slots,
            slots,
            slots,
            slots,
            dma((len(SMALL) + 2 * STATE_PARTS + 14,)),
            dma,
            dma((GROUPS,)),
            dma,
            dma((GROUPS,)),
            pltpu.SemaphoreType.REGULAR,
        ],
        compiler_params=pltpu.CompilerParams(
            collective_id=0, has_side_effects=True, vmem_limit_bytes=42 * 2**20
        ),
        name="layer",
    )(*map(keep, small), *map(keep, wide))


def store_kernel(out_vmem, re_vmem, im_vmem, out_ref, re_ref, im_ref, sem):
    copies = [
        pltpu.make_async_copy(src, dst, sem.at[i])
        for i, (src, dst) in enumerate(
            ((re_vmem, re_ref), (im_vmem, im_ref), (out_vmem, out_ref))
        )
    ]
    for copy in copies:
        copy.start()
    for copy in copies:
        copy.wait()


def store(*arrays):
    return pl.pallas_call(
        store_kernel,
        out_shape=tuple(jax.ShapeDtypeStruct(a.shape, a.dtype) for a in arrays),
        in_specs=[pl.BlockSpec(memory_space=pltpu.VMEM)] * 3,
        out_specs=(pl.BlockSpec(memory_space=pl.ANY),) * 3,
        scratch_shapes=[pltpu.SemaphoreType.DMA((3,))],
        compiler_params=pltpu.CompilerParams(vmem_limit_bytes=2**20),
        name="store",
    )(*arrays)


def per_device(
    residual,
    branch_in,
    state_real,
    state_imag,
    decay_rate,
    frequency,
    log_step,
    input_real,
    input_imag,
    output_matrix_real,
    output_matrix_imaginary,
    skip_gain,
    glu_value,
    glu_gate,
    mix_gain,
    moe_in_gain,
    moe_out_gain,
    routes,
    route_weights,
    expert_gate,
    expert_up,
    expert_down,
    shared_gate,
    shared_up,
    shared_down,
):
    small = (
        log_step.reshape(1, 64),
        decay_rate,
        frequency,
        jnp.transpose(routes),
        jnp.transpose(route_weights),
        branch_in,
        jnp.transpose(input_real, (0, 2, 1)).reshape(1024, 64),
        jnp.transpose(input_imag, (0, 2, 1)).reshape(1024, 64),
        output_matrix_real.reshape(1024, 64),
        output_matrix_imaginary.reshape(1024, 64),
        skip_gain.reshape(1, 1024),
        residual,
        mix_gain.reshape(1, 2048),
        moe_in_gain.reshape(1, 2048),
        moe_out_gain.reshape(1, 2048),
    )
    wide = (
        state_real,
        state_imag,
        glu_value,
        glu_gate,
        expert_gate.reshape(2048, 512),
        expert_up.reshape(2048, 512),
        expert_down.reshape(512, 2048),
        shared_gate,
        shared_up,
        shared_down,
    )
    return store(*layer(small, wide))


def solution(mesh):
    return jax.shard_map(
        per_device,
        mesh=mesh,
        in_specs=(
            P("ep", None),
            P("ep", None),
            P("ep", None),
            P("ep", None),
            P(),
            P(),
            P(),
            P(),
            P(),
            P(),
            P(),
            P(),
            P(),
            P(),
            P(),
            P(),
            P(),
            P("ep", None),
            P("ep", None),
            P("ep", None, None),
            P("ep", None, None),
            P("ep", None, None),
            P(),
            P(),
            P(),
        ),
        out_specs=(P("ep", None), P("ep", None), P("ep", None)),
        check_vma=False,
    )
```
